512 devices in a mesh: sp: 128 (over z, x, core), tp: 4 (over y).
Axes of the slice: x: 4, y: 4, z: 16, core: 2. Of those that a mesh axis runs over, the one named last changes fastest.
Arguments:
- tokens: bfloat16 [65536, 2048], P(('sp', 'tp')), may hold values from -6 to 6
- input_norm_scale: bfloat16 [2048], replicated, may hold values from 0.099609375 to 1.8984375
- outer_gate_weight: bfloat16 [2048, 1024], P('sp', 'tp'), may hold values from -0.125 to 0.125
- inner_gate_weight: bfloat16 [2048, 1024], P('sp', 'tp'), may hold values from -0.125 to 0.125
- value_weight_matrix: bfloat16 [2048, 1024], P('sp', 'tp'), may hold values from -0.125 to 0.125
- output_gate_weight: bfloat16 [2048, 1024], P('sp', 'tp'), may hold values from -0.125 to 0.125
- state_input_weight: bfloat16 [2048, 1024], P('sp', 'tp'), may hold values from -0.125 to 0.125
- write_key_weight: bfloat16 [2048, 512], P('sp', 'tp'), may hold values from -0.125 to 0.125
- read_key_weight: bfloat16 [2048, 512], P('sp', 'tp'), may hold values from -0.125 to 0.125
- step_size_weight: bfloat16 [2048, 16], P(None, 'tp'), may hold values from -0.125 to 0.125
- gated_conv_weight: bfloat16 [3, 1024], P(None, 'tp'), may hold values from -3.5 to 3.5
- input_conv_weight: bfloat16 [4, 1024], P(None, 'tp'), may hold values from -3 to 3
- write_conv_weight: bfloat16 [4, 512], P(None, 'tp'), may hold values from -3 to 3
- read_conv_weight: bfloat16 [4, 512], P(None, 'tp'), may hold values from -3 to 3
- step_size_bias: float32 [16], P('tp'), may hold values from -1 to 0.5
- log_decay_rate: float32 [16], P('tp'), may hold values from -16 to -2.5, as said below
- decay_spikes: float32 [16, 65536], P('tp', 'sp'), may hold values from -1 to 0, as said below
- direct_path_weight: float32 [16], P('tp'), may hold values from 0.5 to 2
- head_norm_scale: bfloat16 [1024], P('tp'), may hold values from 0.099609375 to 1.8984375
- conv_output_weight: bfloat16 [1024, 2048], P('tp', 'sp'), may hold values from -0.125 to 0.125
- state_output_weight: bfloat16 [1024, 2048], P('tp', 'sp'), may hold values from -0.125 to 0.125
Outputs:
- mixed: bfloat16 [65536, 2048], P(('sp', 'tp'))
The draws below stay inside these ranges and needn't reach their ends.
Inputs may be any that keep to these rules, and one draw needn't show every extreme that they name: `log_decay_rate`: one value a head. `decay_spikes`: never positive.
All inputs are finite; a program needn't handle non-finite values.
Results may differ from the reference program's by a relative error of at most 0.017.
Values may be sent and summed in bfloat16 or wider, within the bound.
A program may use at most 128 MiB of HBM per device.

```python
import math
import jax
import jax.numpy as jnp
from jax import lax

D = 2048
CONV = 1024
MIXER_HEADS = 16
HEAD_DIM = 64
GROUPS = 4
STATE = 128
SHORT_K = 3
SSD_K = 4
BLOCK = 64
TOK_DEV = 512
INNER = 1024
SEQUENCE_TOKENS = 65536
N_TP = 4


def draw_tokens(key, part):
    positions = jnp.arange(SEQUENCE_TOKENS, dtype=jnp.int32)
    segment_ids = positions * 8 // SEQUENCE_TOKENS
    jitter_values = jax.random.truncated_normal(jax.random.fold_in(key, 31), -4.5, 4.5, (SEQUENCE_TOKENS, D), jnp.float32)
    directions = jax.random.uniform(jax.random.fold_in(key, 32), (8, D), jnp.float32, -1.2, 1.2)
    offsets = jnp.take(directions, segment_ids, axis=0)
    return (jitter_values + offsets).astype(jnp.bfloat16)


def draw_log_decay_rate(key, part):
    ranking = jax.random.permutation(jax.random.fold_in(key, 11), MIXER_HEADS)
    quick_heads = ranking < MIXER_HEADS // 2
    fast_rates = jnp.exp(jax.random.uniform(jax.random.fold_in(key, 12), (MIXER_HEADS,), jnp.float32, math.log(0.02), math.log(0.08)))
    slow_rates = jnp.exp(jax.random.uniform(jax.random.fold_in(key, 13), (MIXER_HEADS,), jnp.float32, math.log(0.1), math.log(0.3))) / SEQUENCE_TOKENS
    return jnp.log(jnp.where(quick_heads, fast_rates, slow_rates)).astype(jnp.float32)


def draw_decay_spikes(key, part):
    blocks = SEQUENCE_TOKENS // TOK_DEV
    levels = jnp.exp(jax.random.uniform(jax.random.fold_in(key, 21), (MIXER_HEADS, blocks), jnp.float32, math.log(0.25), math.log(2.0)))
    stable_decay = -0.3 / SEQUENCE_TOKENS * jnp.repeat(levels, TOK_DEV, axis=1)
    spike_positions = jax.random.randint(jax.random.fold_in(key, 22), (3,), 0, SEQUENCE_TOKENS)
    spike_present = jnp.any(jnp.arange(SEQUENCE_TOKENS)[None, :] == spike_positions[:, None], axis=0)
    spike_decrement = jax.random.uniform(jax.random.fold_in(key, 23), (MIXER_HEADS, SEQUENCE_TOKENS), jnp.float32, 0.22, 0.69)
    return (stable_decay - jnp.where(spike_present[None, :], spike_decrement, 0.0)).astype(jnp.float32)


def steps_of(own_key, dims, pieces, least, largest):
    level, own = 1.0, jax.random.fold_in(own_key, 6)
    for dim, parts in pieces:
        draws = jnp.exp(jax.random.uniform(jax.random.fold_in(own, dim), (parts,), jnp.float32, least / len(pieces), largest / len(pieces)))
        level = level * jnp.repeat(draws, dims[dim] // parts).reshape([-1 if axis == dim else 1 for axis in range(len(dims))])
    return level


def gaussian(rng, shape, deviation, limit, pieces=(), kind=jnp.bfloat16):
    drawn = jax.random.normal(rng, shape, jnp.float32) * deviation
    if len(pieces) > 0:
        drawn = steps_of(rng, shape, pieces, -0.22, 0.18) * drawn
    return jnp.clip(drawn, min=-limit, max=limit).astype(kind)


def setup_inputs(seed: int = 0) -> dict:
    streams_of = jax.random.split(jax.random.key(seed), 22)
    return {
        "tokens": draw_tokens(jax.random.fold_in(streams_of[21], 71), 0),
        "input_norm_scale": jnp.clip(1.0 + 0.18 * jax.random.normal(streams_of[1], (D,), jnp.float32), 0.099609375, 1.8984375).astype(jnp.bfloat16),
        "outer_gate_weight": gaussian(streams_of[2], (D, CONV), D ** -0.5, 0.125, ((0, 128), (1, 4))),
        "inner_gate_weight": gaussian(streams_of[3], (D, CONV), D ** -0.5, 0.125, ((0, 128), (1, 4))),
        "value_weight_matrix": gaussian(streams_of[4], (D, CONV), D ** -0.5, 0.125, ((0, 128), (1, 4))),
        "output_gate_weight": gaussian(streams_of[5], (D, INNER), D ** -0.5, 0.125, ((0, 128), (1, 4))),
        "state_input_weight": gaussian(streams_of[6], (D, INNER), D ** -0.5, 0.125, ((0, 128), (1, 4))),
        "write_key_weight": gaussian(streams_of[7], (D, GROUPS * STATE), D ** -0.5, 0.125, ((0, 128), (1, 4))),
        "read_key_weight": gaussian(streams_of[8], (D, GROUPS * STATE), D ** -0.5, 0.125, ((0, 128), (1, 4))),
        "step_size_weight": gaussian(streams_of[9], (D, MIXER_HEADS), D ** -0.5, 0.125, ((1, 4),)),
        "gated_conv_weight": gaussian(streams_of[10], (SHORT_K, CONV), SHORT_K ** -0.5, 3.5, ((1, 4),)),
        "input_conv_weight": gaussian(streams_of[11], (SSD_K, INNER), SSD_K ** -0.5, 3.0, ((1, 4),)),
        "write_conv_weight": gaussian(streams_of[12], (SSD_K, GROUPS * STATE), SSD_K ** -0.5, 3.0, ((1, 4),)),
        "read_conv_weight": gaussian(streams_of[13], (SSD_K, GROUPS * STATE), SSD_K ** -0.5, 3.0, ((1, 4),)),
        "step_size_bias": jnp.clip(-1.0 + 1.5 * jax.random.uniform(streams_of[14], (MIXER_HEADS,), jnp.float32) ** steps_of(streams_of[14], (MIXER_HEADS,), ((0, 4),), -0.2, 0.2), -1.0, 0.5),
        "log_decay_rate": draw_log_decay_rate(jax.random.fold_in(streams_of[21], 71), 0),
        "decay_spikes": draw_decay_spikes(jax.random.fold_in(streams_of[21], 71), 0),
        "direct_path_weight": jnp.clip(0.5 + 1.5 * jax.random.uniform(streams_of[17], (MIXER_HEADS,), jnp.float32) ** steps_of(streams_of[17], (MIXER_HEADS,), ((0, 4),), -0.2, 0.2), 0.5, 2.0),
        "head_norm_scale": jnp.clip(1.0 + 0.18 * jax.random.normal(streams_of[18], (INNER,), jnp.float32), 0.099609375, 1.8984375).astype(jnp.bfloat16),
        "conv_output_weight": gaussian(streams_of[19], (CONV, D), (CONV + INNER) ** -0.5, 0.125, ((0, 4), (1, 128))),
        "state_output_weight": gaussian(streams_of[20], (INNER, D), (CONV + INNER) ** -0.5, 0.125, ((0, 4), (1, 128))),
    }


epsilon = 1e-05
highest = lax.Precision.HIGHEST

def causal_taps(values, tap_weights):
    tap_count = tap_weights.shape[0]
    length = values.shape[0]
    padded = jnp.concatenate([jnp.zeros((tap_count - 1, values.shape[1]), jnp.float32), values], axis=0)
    running = tap_weights[0] * padded[0:length]
    for offset in range(1, tap_count):
        running = running + tap_weights[offset] * padded[offset:offset + length]
    return running

def reference(tokens, input_norm_scale, outer_gate_weight, inner_gate_weight, value_weight_matrix, output_gate_weight, state_input_weight, write_key_weight, read_key_weight, step_size_weight, gated_conv_weight, input_conv_weight, write_conv_weight, read_conv_weight, step_size_bias, log_decay_rate, decay_spikes, direct_path_weight, head_norm_scale, conv_output_weight, state_output_weight):
    token_rows = tokens.astype(jnp.float32)
    scaled = token_rows * lax.rsqrt(lax.optimization_barrier(jnp.mean(token_rows * token_rows, axis=1, keepdims=True)) + epsilon)
    normed = (scaled * input_norm_scale.astype(jnp.float32)).astype(jnp.bfloat16)

    def project(weight):
        return jnp.dot(normed, weight, preferred_element_type=jnp.float32).astype(jnp.bfloat16)
    outer_gate = project(outer_gate_weight)
    inner_gate = project(inner_gate_weight)
    conv_input = project(value_weight_matrix)
    out_gate = project(output_gate_weight)
    state_input = project(state_input_weight)
    write_keys = project(write_key_weight)
    read_keys = project(read_key_weight)
    step_raw = jnp.dot(normed, step_size_weight, preferred_element_type=jnp.float32)
    product = inner_gate.astype(jnp.float32) * conv_input.astype(jnp.float32)
    mixer_part = (outer_gate.astype(jnp.float32) * causal_taps(product, gated_conv_weight.astype(jnp.float32))).astype(jnp.bfloat16)
    seq_input = jax.nn.silu(causal_taps(state_input.astype(jnp.float32), input_conv_weight.astype(jnp.float32)))
    seq_write = jax.nn.silu(causal_taps(write_keys.astype(jnp.float32), write_conv_weight.astype(jnp.float32)))
    seq_read = jax.nn.silu(causal_taps(read_keys.astype(jnp.float32), read_conv_weight.astype(jnp.float32)))
    discrete_step = jax.nn.softplus(step_raw + step_size_bias[None, :])
    step_logarithm = discrete_step * (-jnp.exp(log_decay_rate))[None, :] + decay_spikes.T
    blocks = SEQUENCE_TOKENS // BLOCK
    per_group = MIXER_HEADS // GROUPS
    input_blocks = seq_input.reshape(blocks, BLOCK, MIXER_HEADS, HEAD_DIM)
    weighted = input_blocks * discrete_step.reshape(blocks, BLOCK, MIXER_HEADS, 1)
    write_blocks = seq_write.reshape(blocks, BLOCK, GROUPS, STATE)
    read_blocks = seq_read.reshape(blocks, BLOCK, GROUPS, STATE)
    cumulative = jnp.cumsum(step_logarithm.reshape(blocks, BLOCK, MIXER_HEADS), axis=1)
    causal = lax.broadcasted_iota(jnp.int32, (BLOCK, BLOCK), 0) >= lax.broadcasted_iota(jnp.int32, (BLOCK, BLOCK), 1)

    def one_block(carried_state, inputs):
        block_weighted, block_write, block_read, block_cum = inputs
        write_heads = jnp.repeat(block_write, per_group, axis=1)
        read_heads = jnp.repeat(block_read, per_group, axis=1)
        scores = jnp.einsum('lhm,shm->lsh', read_heads, write_heads, precision=highest)
        damping = jnp.exp(jnp.where(causal[:, :, None], block_cum[:, None, :] - block_cum[None, :, :], -jnp.inf))
        within = jnp.einsum('lsh,shp->lhp', scores * damping, block_weighted, precision=highest)
        from_before = jnp.einsum('lhm,hpm->lhp', read_heads, carried_state, precision=highest) * jnp.exp(block_cum)[:, :, None]
        to_end = jnp.exp(block_cum[-1:, :] - block_cum)
        new_state = jnp.einsum('shm,shp->hpm', write_heads * to_end[:, :, None], block_weighted, precision=highest)
        return (carried_state * jnp.exp(block_cum[-1])[:, None, None] + new_state, within + from_before)
    _, block_outputs = lax.scan(one_block, jnp.zeros((MIXER_HEADS, HEAD_DIM, STATE), jnp.float32), (weighted, write_blocks, read_blocks, cumulative))
    head_out = block_outputs + direct_path_weight[None, None, :, None] * input_blocks
    head_out = head_out.reshape(SEQUENCE_TOKENS, MIXER_HEADS * HEAD_DIM)
    gated_heads = (head_out * jax.nn.silu(out_gate.astype(jnp.float32))).reshape(SEQUENCE_TOKENS, MIXER_HEADS, HEAD_DIM)
    normalized = gated_heads * lax.rsqrt(lax.optimization_barrier(jnp.mean(gated_heads * gated_heads, axis=2, keepdims=True)) + epsilon)
    state_part = (normalized.reshape(SEQUENCE_TOKENS, MIXER_HEADS * HEAD_DIM) * head_norm_scale.astype(jnp.float32)).astype(jnp.bfloat16)
    share_conv = CONV // N_TP
    share_state = MIXER_HEADS * HEAD_DIM // N_TP
    running = jnp.zeros((SEQUENCE_TOKENS, D), jnp.float32)
    for head_block in range(N_TP):
        conv_slice = slice(head_block * share_conv, (head_block + 1) * share_conv)
        state_slice = slice(head_block * share_state, (head_block + 1) * share_state)
        partial_sum = jnp.dot(mixer_part[:, conv_slice], conv_output_weight[conv_slice], preferred_element_type=jnp.float32)
        partial_sum = partial_sum + jnp.dot(state_part[:, state_slice], state_output_weight[state_slice], preferred_element_type=jnp.float32)
        rounded = lax.optimization_barrier(partial_sum.astype(jnp.bfloat16))
        running = running + rounded.astype(jnp.float32)
    return running.astype(jnp.bfloat16)
```

```python
import functools

import jax
import jax.numpy as jnp
from jax import lax
from jax.experimental import pallas as pl
from jax.experimental.pallas import tpu as pltpu
from jax.sharding import Mesh
from jax.sharding import PartitionSpec as P

SP = ("sp_0", "sp_1", "sp_2")
SP_TP = ("sp_0", "sp_1", "sp_2", "tp")
NZ, NX, NC, NY = 16, 4, 2, 4
PLANE = NX * NC
D = 2048
ROWS = 16
W = 256
STATE = 128
HEADS = 4
HEAD_DIM = 64
OWN = 128
LEN = 512
RIM = 16
L = 128
BLOCKS = LEN // L
NA = 5
GROUPS = 8
OUTER, INNER, VALUE, CONV_T, STATE_T, OUT_GATE, STATE_IN, KEYS = range(8)
EPS = 1e-05
MESH = pl.DeviceIdType.MESH
F32 = jnp.float32
BF16 = jnp.bfloat16
HIGH = lax.Precision.HIGHEST


def silu(v):
    return v / (1.0 + jnp.exp(-v))


def dot_nn(a, b, precision=None):
    return lax.dot_general(
        a, b, (((1,), (0,)), ((), ())), precision=precision, preferred_element_type=F32
    )


def dot_nt(a, b, precision=None):
    return lax.dot_general(
        a, b, (((1,), (1,)), ((), ())), precision=precision, preferred_element_type=F32
    )


def dot_tn(a, b, precision=None):
    return lax.dot_general(
        a, b, (((0,), (0,)), ((), ())), precision=precision, preferred_element_type=F32
    )


def iota(shape, dim):
    return lax.broadcasted_iota(jnp.int32, shape, dim)


def layer_kernel(
    tok,
    scale,
    outer_w,
    inner_w,
    value_w,
    out_gate_w,
    state_in_w,
    write_w,
    read_w,
    step_w,
    gated_taps,
    input_taps,
    write_taps,
    read_taps,
    bias,
    rate,
    spikes,
    direct,
    head_scale,
    conv_out_w,
    state_out_w,
    out,
    wbuf,
    nb,
    pj,
    product,
    mixer,
    spart,
    xin,
    wk,
    rk,
    within,
    cumx,
    before,
    decay,
    s_own,
    s1,
    pref,
    s2_own,
    s2,
    zin,
    s3_own,
    s3,
    t_own,
    t_plane,
    tz_own,
    t_z,
    rs_far,
    rs_right,
    rs_left,
    got_far_l,
    got_far_r,
    got_left,
    got_right,
    tok_s,
    tok_r,
    az_s,
    azl_r,
    azr_r,
    ax_s,
    axl_r,
    axr_r,
    axfl_r,
    axfr_r,
    bx_s,
    bx_r,
    bz_s,
    bzl_r,
    bzr_r,
    dd_s,
    dd_r,
    rim_s,
    rim_r,
    st_s,
    st_r,
    s2_s,
    s2_r,
    rs_s,
    rs_r,
):
    z = lax.axis_index("sp_0")
    x = lax.axis_index("sp_1")
    c = lax.axis_index("sp_2")
    y = lax.axis_index("tp")
    p = x * NC + c
    sp = z * PLANE + p

    def zm(k):
        return lax.rem(z + (k + NZ), NZ)

    def xm(k):
        return lax.rem(x + (k + NX), NX)

    def ym(k):
        return lax.rem(y + (k + NY), NY)

    def in_plane(k):
        q = lax.rem(p + k, PLANE)
        return q, (z, q // NC, lax.rem(q, NC), y)

    z_right, z_left = (zm(1), x, c, y), (zm(-1), x, c, y)
    x_right, x_left = (z, xm(1), c, y), (z, xm(-1), c, y)
    y_right, y_left = (z, x, c, ym(1)), (z, x, c, ym(-1))
    partner = (z, x, 1 - c, y)

    def along(k):
        q = lax.rem(sp + (k + NZ * PLANE), NZ * PLANE)
        r = lax.rem(q, PLANE)
        return (q // PLANE, r // NC, lax.rem(r, NC), y)

    barrier = pltpu.get_barrier_semaphore()

    def hello(where):
        pl.semaphore_signal(barrier, inc=1, device_id=where, device_id_type=MESH)

    hello(y_right)
    hello(y_left)
    hello(along(-1))

    def hello_plane(k, carry):
        hello(in_plane(k)[1])
        return carry

    def hello_z(k, carry):
        hello((lax.rem(z + k, NZ), x, c, y))
        return carry

    lax.fori_loop(1, PLANE, hello_plane, 0)
    lax.fori_loop(1, NZ, hello_z, 0)

    def send(src, dst, s_sem, r_sem, where):
        pltpu.make_async_remote_copy(
            src_ref=src,
            dst_ref=dst,
            send_sem=s_sem,
            recv_sem=r_sem,
            device_id=where,
            device_id_type=MESH,
        ).start()

    def wait(ref, sem):
        pltpu.make_async_copy(ref, ref, sem).wait()

    for group, ref in (
        (OUTER, outer_w),
        (INNER, inner_w),
        (VALUE, value_w),
        (OUT_GATE, out_gate_w),
        (STATE_IN, state_in_w),
    ):
        wbuf[group, z, x, c] = ref[...]
    wbuf[KEYS, z, x, c, :, 0:STATE] = write_w[...]
    wbuf[KEYS, z, x, c, :, STATE:W] = read_w[...]
    eye = (iota((W, W), 0) == iota((W, W), 1)).astype(BF16)
    wbuf[CONV_T, z, x, c] = dot_tn(conv_out_w[...], eye).astype(BF16)
    wbuf[STATE_T, z, x, c] = dot_tn(state_out_w[...], eye).astype(BF16)

    token_rows = tok[...].astype(F32)
    scaled = token_rows * lax.rsqrt(
        jnp.mean(token_rows * token_rows, axis=1, keepdims=True) + EPS
    )
    own_row = pl.multiple_of(RIM + y * OWN, RIM)
    nb[pl.ds(own_row, OWN)] = (scaled * scale[...].astype(F32)).astype(BF16)

    pl.semaphore_wait(barrier, 2 + 1 + (PLANE - 1) + (NZ - 1))

    HALF = OWN // 2

    def tok_piece(k, half):
        start = pl.multiple_of(RIM + ym(k) * OWN + half * HALF, RIM)
        return nb.at[pl.ds(start, HALF)]

    def send_tok(k, half, index, where):
        piece = tok_piece(k, half)
        send(piece, piece, tok_s.at[index], tok_r.at[index], where)

    def a_block(zz, xx):
        return wbuf.at[pl.ds(0, NA), zz, xx, c]

    def a_half(zz, xx, half):
        return wbuf.at[pl.ds(0, NA), zz, xx, c, :, pl.ds(half * 128, 128)]

    def b_block(xx):
        return wbuf.at[pl.ds(NA, GROUPS - NA), z, xx, c]

    def b_half(xx, half):
        return wbuf.at[pl.ds(NA, GROUPS - NA), z, xx, c, :, pl.ds(half * 128, 128)]

    def b_chunk(group, zz):
        return wbuf.at[group, zz, :, c]

    send(b_block(x), b_block(x), bx_s.at[0], bx_r.at[0], x_right)
    send(b_block(x), b_block(x), bx_s.at[1], bx_r.at[1], x_left)
    send_tok(0, 0, 0, y_right)
    send_tok(0, 1, 1, y_left)
    send_tok(0, 1, 2, y_right)
    send_tok(0, 0, 3, y_left)

    def az_send(k_right, k_left, step):
        if step <= 7:
            blk = a_block(zm(k_right), x)
            send(blk, blk, az_s, azl_r.at[step], z_right)
        if step <= 6:
            blk = a_block(zm(k_left), x)
            send(blk, blk, az_s, azr_r.at[step], z_left)

    def offsets(s):
        if s == 0:
            return [(0, 0)]
        found = [(-s, 0)]
        if s <= 7:
            found.append((s, 1))
        return found

    def ax_send(s):
        for k, side in offsets(s):
            i = 2 * s + side
            blk = a_block(zm(k), x)
            send(blk, blk, ax_s, axl_r.at[i], x_right)
            send(blk, blk, ax_s, axr_r.at[i], x_left)

    def ax_forward(s):
        for k, side in offsets(s):
            i = 2 * s + side
            wait(a_block(zm(k), xm(-1)), axl_r.at[i])
            half = a_half(zm(k), xm(-1), 0)
            send(half, half, ax_s, axfl_r.at[i], x_right)
            wait(a_block(zm(k), xm(1)), axr_r.at[i])
            half = a_half(zm(k), xm(1), 1)
            send(half, half, ax_s, axfr_r.at[i], x_left)

    def a_across(s):
        for k, side in offsets(s):
            i = 2 * s + side
            wait(a_half(zm(k), xm(2), 0), axfl_r.at[i])
            wait(a_half(zm(k), xm(2), 1), axfr_r.at[i])
            blk = wbuf.at[pl.ds(0, NA), zm(k), :, c]
            send(blk, blk, dd_s.at[0], dd_r.at[0], partner)

    def bz_send(k_right, k_left, step, group):
        b = group - NA
        if step <= 7:
            blk = b_chunk(group, zm(k_right))
            send(blk, blk, bz_s, bzl_r.at[b * 8 + step], z_right)
        if step <= 6:
            blk = b_chunk(group, zm(k_left))
            send(blk, blk, bz_s, bzr_r.at[b * 8 + step], z_left)

    def b_across(group, k):
        blk = b_chunk(group, zm(k))
        send(blk, blk, dd_s.at[1 + group - NA], dd_r.at[1 + group - NA], partner)

    order_b = (KEYS, STATE_IN, OUT_GATE)

    def b_round(s):
        for group in order_b:
            b = group - NA
            wait(b_chunk(group, zm(-s)), bzl_r.at[b * 8 + s - 1])
            if s <= 7:
                wait(b_chunk(group, zm(s)), bzr_r.at[b * 8 + s - 1])
            bz_send(-s, s, s, group)
            b_across(group, -s)
            if s <= 7:
                b_across(group, s)

    az_send(0, 0, 0)
    ax_send(0)
    wait(b_block(xm(-1)), bx_r.at[0])
    send(b_half(xm(-1), 0), b_half(xm(-1), 0), bx_s.at[2], bx_r.at[2], x_right)
    wait(b_block(xm(1)), bx_r.at[1])
    send(b_half(xm(1), 1), b_half(xm(1), 1), bx_s.at[3], bx_r.at[3], x_left)
    wait(b_half(xm(2), 0), bx_r.at[2])
    wait(b_half(xm(2), 1), bx_r.at[3])
    for group in order_b:
        bz_send(0, 0, 0, group)
    for group in order_b:
        b_across(group, 0)

    for s in range(1, 9):
        wait(a_block(zm(-s), x), azl_r.at[s - 1])
        if s <= 7:
            wait(a_block(zm(s), x), azr_r.at[s - 1])
        az_send(-s, s, s)
        ax_send(s)
        ax_forward(s - 1)
        if s >= 2:
            a_across(s - 2)
        b_round(s)
        if s == 2:
            wait(tok_piece(-1, 0), tok_r.at[0])
            send_tok(-1, 0, 4, y_right)
            wait(tok_piece(1, 1), tok_r.at[1])
            send_tok(1, 1, 5, y_left)
    ax_forward(8)
    a_across(7)

    wait(tok_piece(-1, 1), tok_r.at[2])
    wait(tok_piece(1, 0), tok_r.at[3])
    wait(tok_piece(2, 0), tok_r.at[4])
    wait(tok_piece(2, 1), tok_r.at[5])

    @pl.when(sp < NZ * PLANE - 1)
    def _():
        send(nb.at[pl.ds(LEN, RIM)], nb.at[pl.ds(0, RIM)], rim_s, rim_r, along(1))

    @pl.when(sp == 0)
    def _():
        nb[0:RIM] = jnp.zeros((RIM, D), BF16)

    step_raw = dot_nt(step_w[...], nb[RIM : RIM + LEN])
    head_row = iota((HEADS, LEN), 0)

    def per_head(ref, index):
        return functools.reduce(
            lambda got, h: jnp.where(index == h, ref[h], got),
            range(1, HEADS),
            jnp.full(index.shape, ref[0], F32),
        )

    shifted = step_raw + per_head(bias, head_row)
    step = jnp.maximum(shifted, 0.0) + jnp.log1p(jnp.exp(-jnp.abs(shifted)))
    log_step = step * (-jnp.exp(per_head(rate, head_row))) + spikes[...]
    ramp = (iota((L, L), 0) <= iota((L, L), 1)).astype(F32)
    spread = (iota((HEADS, W), 1) // HEAD_DIM == iota((HEADS, W), 0)).astype(F32)
    total = jnp.zeros((1, W), F32)
    cum_rows = []
    for b in range(BLOCKS):
        rows = dot_nn(log_step[:, b * L : (b + 1) * L], ramp, HIGH)
        cum_rows.append(rows)
        wide = dot_tn(rows, spread, HIGH)
        cumx[b] = wide
        decay[b] = wide[L - 1 : L]
        total = total + wide[L - 1 : L]
    t_own[0] = total

    for k in range(1, PLANE):
        _, where = in_plane(k)
        send(t_own, t_plane.at[pl.ds(p, 1)], st_s.at[0], st_r.at[0], where)
    t_plane[p] = total

    a_across(8)
    wait(t_plane.at[pl.ds(0, PLANE - 1)], st_r.at[0])
    tz_own[0] = jnp.sum(t_plane[...], axis=0)

    def send_tz(k, carry):
        there = lax.rem(z + k, NZ)
        send(tz_own, t_z.at[pl.ds(z, 1)], st_s.at[1], st_r.at[1], (there, x, c, y))
        return carry

    lax.fori_loop(1, NZ, send_tz, 0)

    @pl.when(sp > 0)
    def _():
        wait(nb.at[pl.ds(0, RIM)], rim_r)

    for b in range(GROUPS - NA):
        wait(wbuf.at[NA + b, :, :, 1 - c], dd_r.at[1 + b])

    def project(group, carry):
        acc = dot_nn(nb[...], wbuf[group].reshape(D, W))
        pj[group] = acc.astype(BF16).astype(F32)
        return carry

    lax.fori_loop(STATE_IN, KEYS + 1, project, 0)

    def causal(ref, taps, first, last):
        count = taps.shape[0]
        weights = taps[...].astype(F32)
        start = RIM - count + 1
        running = weights[0:1] * ref[start : start + LEN, first:last]
        for k in range(1, count):
            running = running + weights[k : k + 1] * ref[start + k : start + k + LEN, first:last]
        return running

    xin[...] = silu(causal(pj.at[STATE_IN], input_taps, 0, W))
    wk[...] = silu(causal(pj.at[KEYS], write_taps, 0, STATE)).astype(BF16)
    rk[...] = silu(causal(pj.at[KEYS], read_taps, STATE, W)).astype(BF16)

    state = jnp.zeros((STATE, W), F32)
    lane_head = iota((L, W), 1) // HEAD_DIM
    spread_l = (iota((HEADS, HEADS * L), 1) // L == iota((HEADS, HEADS * L), 0)).astype(F32)
    keep = iota((L, HEADS * L), 0) >= lax.rem(iota((L, HEADS * L), 1), L)
    weighted = []
    for b in range(BLOCKS):
        steps = dot_tn(step[:, b * L : (b + 1) * L], spread, HIGH)
        heavy = xin[b * L : (b + 1) * L] * steps
        weighted.append(heavy.astype(BF16))
        to_end = jnp.exp(decay[b] - cumx[b])
        own = dot_tn(wk[b * L : (b + 1) * L], (heavy * to_end).astype(BF16))
        before[b] = state
        state = state * jnp.exp(decay[b]) + own
    s_own[...] = state.astype(BF16).reshape(PLANE, ROWS, W)
    for k in range(1, PLANE):
        q, where = in_plane(k)
        send(s_own.at[q], s1.at[p], st_s.at[2], st_r.at[2], where)
    s1[p] = s_own[p]

    def within_block(b):
        rows = slice(b * L, (b + 1) * L)
        scores = dot_nt(rk[rows], wk[rows])
        cols = dot_tn(cum_rows[b], spread_l, HIGH)
        flat = jnp.concatenate([cum_rows[b][h : h + 1] for h in range(HEADS)], axis=1)
        damping = jnp.exp(jnp.where(keep, cols - flat, -jnp.inf))
        mixed = (jnp.concatenate([scores] * HEADS, axis=1) * damping).astype(BF16)
        stacked = jnp.concatenate(
            [jnp.where(lane_head == h, weighted[b], jnp.zeros_like(weighted[b])) for h in range(HEADS)],
            axis=0,
        )
        within[rows] = dot_nn(mixed, stacked)

    for b in range(BLOCKS):
        within_block(b)

    wait(s1.at[pl.ds(0, PLANE - 1)], st_r.at[2])
    running = jnp.zeros((ROWS, W), F32)
    for i in range(PLANE):
        pref[i] = running
        running = running * jnp.exp(t_plane[i]) + s1[i].astype(F32)
    s2_own[...] = running.astype(BF16)

    def send_s2(k, carry):
        @pl.when(z + k < NZ)
        def _():
            send(s2_own, s2.at[z], s2_s.at[k], s2_r.at[z], (z + k, x, c, y))

        return carry

    lax.fori_loop(1, NZ, send_s2, 0)

    wait(wbuf.at[pl.ds(0, NA), :, :, 1 - c], dd_r.at[0])
    lax.fori_loop(OUTER, VALUE + 1, project, 0)
    lax.fori_loop(OUT_GATE, OUT_GATE + 1, project, 0)
    product[...] = pj[INNER] * pj[VALUE]
    mixer[...] = (pj[OUTER, RIM : RIM + LEN] * causal(product, gated_taps, 0, W)).astype(BF16)

    wait(t_z.at[pl.ds(0, NZ - 1)], st_r.at[1])
    zin[...] = jnp.zeros((ROWS, W), F32)

    def take_s2(k, carry):
        @pl.when(k < z)
        def _():
            wait(s2.at[k], s2_r.at[k])
            zin[...] = zin[...] * jnp.exp(t_z[k]) + s2[k].astype(F32)

        return carry

    lax.fori_loop(0, NZ - 1, take_s2, 0)
    arriving = zin[...]
    logs = jnp.zeros((1, W), F32)
    for i in range(PLANE):
        s3_own[i] = (pref[i] + arriving * jnp.exp(logs)).astype(BF16)
        logs = logs + t_plane[i]
    for k in range(1, PLANE):
        q, where = in_plane(k)
        send(s3_own.at[q], s3.at[p], st_s.at[3], st_r.at[3], where)
    s3[p] = s3_own[p]

    lane = iota((1, W), 1) // HEAD_DIM
    direct_row = per_head(direct, lane)
    same_head = (iota((W, W), 0) // HEAD_DIM == iota((W, W), 1) // HEAD_DIM).astype(F32) * (
        1.0 / HEAD_DIM
    )
    gate = silu(pj[OUT_GATE, RIM : RIM + LEN])
    pj[OUT_GATE, RIM : RIM + LEN] = gate

    wait(s3.at[pl.ds(0, PLANE - 1)], st_r.at[3])
    entering = s3[...].reshape(STATE, W).astype(F32)
    logs = jnp.zeros((1, W), F32)
    for b in range(BLOCKS):
        rows = slice(b * L, (b + 1) * L)
        enter = (before[b] + jnp.exp(logs) * entering).astype(BF16)
        logs = logs + decay[b]
        head_out = (
            within[rows]
            + dot_nn(rk[rows], enter) * jnp.exp(cumx[b])
            + direct_row * xin[rows]
        )
        gated = head_out * pj[OUT_GATE, RIM + b * L : RIM + (b + 1) * L]
        mean = dot_nn(gated * gated, same_head, HIGH)
        spart[rows] = (gated * lax.rsqrt(mean + EPS) * head_scale[...].astype(F32)).astype(BF16)

    def partial(k):
        start = pl.multiple_of(ym(k) * OWN, OWN)
        return dot_nt(mixer[pl.ds(start, OWN)], wbuf[CONV_T].reshape(D, W)) + dot_nt(
            spart[pl.ds(start, OWN)], wbuf[STATE_T].reshape(D, W)
        )

    rs_far[...] = partial(2).astype(BF16)
    send(rs_far.at[0:HALF], got_far_l, rs_s.at[0], rs_r.at[0], y_right)
    send(rs_far.at[HALF:OWN], got_far_r, rs_s.at[1], rs_r.at[1], y_left)
    to_right = partial(1)
    rs_right[HALF:OWN] = to_right[HALF:OWN].astype(BF16)
    send(rs_right.at[HALF:OWN], got_left.at[HALF:OWN], rs_s.at[2], rs_r.at[2], y_right)
    to_left = partial(-1)
    rs_left[0:HALF] = to_left[0:HALF].astype(BF16)
    send(rs_left.at[0:HALF], got_right.at[0:HALF], rs_s.at[3], rs_r.at[3], y_left)
    wait(got_far_l, rs_r.at[0])
    rs_right[0:HALF] = (to_right[0:HALF] + got_far_l[...].astype(F32)).astype(BF16)
    send(rs_right.at[0:HALF], got_left.at[0:HALF], rs_s.at[4], rs_r.at[4], y_right)
    wait(got_far_r, rs_r.at[1])
    rs_left[HALF:OWN] = (to_left[HALF:OWN] + got_far_r[...].astype(F32)).astype(BF16)
    send(rs_left.at[HALF:OWN], got_right.at[HALF:OWN], rs_s.at[5], rs_r.at[5], y_left)
    mine = partial(0)

    for index, half in ((0, 0), (1, 1), (2, 1), (3, 0)):
        wait(tok_piece(0, half), tok_s.at[index])
    wait(tok_piece(-1, 0), tok_s.at[4])
    wait(tok_piece(1, 1), tok_s.at[5])
    wait(wbuf.at[pl.ds(0, NA), pl.ds(0, NZ - 1), 0, 0], az_s)
    wait(wbuf.at[pl.ds(0, NA), :, pl.ds(0, 3), 0], ax_s)
    wait(b_block(x), bx_s.at[0])
    wait(b_block(x), bx_s.at[1])
    wait(b_half(x, 0), bx_s.at[2])
    wait(b_half(x, 1), bx_s.at[3])
    wait(wbuf.at[pl.ds(NA, GROUPS - NA), pl.ds(0, NZ - 1), :, 0], bz_s)
    wait(wbuf.at[pl.ds(0, NA), :, :, c], dd_s.at[0])
    for b in range(GROUPS - NA):
        wait(wbuf.at[NA + b, :, :, c], dd_s.at[1 + b])

    @pl.when(sp < NZ * PLANE - 1)
    def _():
        wait(nb.at[pl.ds(LEN, RIM)], rim_s)

    wait(t_plane.at[pl.ds(0, PLANE - 1)], st_s.at[0])
    wait(t_z.at[pl.ds(0, NZ - 1)], st_s.at[1])
    wait(s_own.at[pl.ds(0, PLANE - 1)], st_s.at[2])
    wait(s3_own.at[pl.ds(0, PLANE - 1)], st_s.at[3])

    def left_s2(k, carry):
        @pl.when(z + k < NZ)
        def _():
            wait(s2_own, s2_s.at[k])

        return carry

    lax.fori_loop(1, NZ, left_s2, 0)
    wait(rs_far.at[0:HALF], rs_s.at[0])
    wait(rs_far.at[HALF:OWN], rs_s.at[1])
    wait(rs_right.at[HALF:OWN], rs_s.at[2])
    wait(rs_left.at[0:HALF], rs_s.at[3])
    wait(rs_right.at[0:HALF], rs_s.at[4])
    wait(rs_left.at[HALF:OWN], rs_s.at[5])

    wait(got_left.at[HALF:OWN], rs_r.at[2])
    wait(got_right.at[0:HALF], rs_r.at[3])
    wait(got_left.at[0:HALF], rs_r.at[4])
    wait(got_right.at[HALF:OWN], rs_r.at[5])
    out[...] = (mine + got_left[...].astype(F32) + got_right[...].astype(F32)).astype(BF16)


def per_device(
    tokens,
    input_norm_scale,
    outer_gate_weight,
    inner_gate_weight,
    value_weight_matrix,
    output_gate_weight,
    state_input_weight,
    write_key_weight,
    read_key_weight,
    step_size_weight,
    gated_conv_weight,
    input_conv_weight,
    write_conv_weight,
    read_conv_weight,
    step_size_bias,
    log_decay_rate,
    decay_spikes,
    direct_path_weight,
    head_norm_scale,
    conv_output_weight,
    state_output_weight,
):
    vmem = pl.BlockSpec(memory_space=pltpu.VMEM)
    smem = pl.BlockSpec(memory_space=pltpu.SMEM)
    dma = pltpu.SemaphoreType.DMA
    return pl.pallas_call(
        layer_kernel,
        out_shape=jax.ShapeDtypeStruct((OWN, D), BF16),
        in_specs=[vmem] * 14 + [smem, smem, vmem, smem] + [vmem] * 3,
        out_specs=vmem,
        scratch_shapes=[
            pltpu.VMEM((GROUPS, NZ, NX, NC, ROWS, W), BF16),
            pltpu.VMEM((RIM + LEN, D), BF16),
            pltpu.VMEM((GROUPS, RIM + LEN, W), F32),
            pltpu.VMEM((RIM + LEN, W), F32),
            pltpu.VMEM((LEN, W), BF16),
            pltpu.VMEM((LEN, W), BF16),
            pltpu.VMEM((LEN, W), F32),
            pltpu.VMEM((LEN, STATE), BF16),
            pltpu.VMEM((LEN, STATE), BF16),
            pltpu.VMEM((LEN, W), F32),
            pltpu.VMEM((BLOCKS, L, W), F32),
            pltpu.VMEM((BLOCKS, STATE, W), F32),
            pltpu.VMEM((BLOCKS, 1, W), F32),
            pltpu.VMEM((PLANE, ROWS, W), BF16),
            pltpu.VMEM((PLANE, ROWS, W), BF16),
            pltpu.VMEM((PLANE, ROWS, W), F32),
            pltpu.VMEM((ROWS, W), BF16),
            pltpu.VMEM((NZ, ROWS, W), BF16),
            pltpu.VMEM((ROWS, W), F32),
            pltpu.VMEM((PLANE, ROWS, W), BF16),
            pltpu.VMEM((PLANE, ROWS, W), BF16),
            pltpu.VMEM((1, 1, W), F32),
            pltpu.VMEM((PLANE, 1, W), F32),
            pltpu.VMEM((1, 1, W), F32),
            pltpu.VMEM((NZ, 1, W), F32),
            pltpu.VMEM((OWN, D), BF16),
            pltpu.VMEM((OWN, D), BF16),
            pltpu.VMEM((OWN, D), BF16),
            pltpu.VMEM((OWN // 2, D), BF16),
            pltpu.VMEM((OWN // 2, D), BF16),
            pltpu.VMEM((OWN, D), BF16),
            pltpu.VMEM((OWN, D), BF16),
            dma((6,)),
            dma((6,)),
            dma,
            dma((8,)),
            dma((8,)),
            dma,
            dma((18,)),
            dma((18,)),
            dma((18,)),
            dma((18,)),
            dma((4,)),
            dma((4,)),
            dma,
            dma((24,)),
            dma((24,)),
            dma((4,)),
            dma((4,)),
            dma,
            dma,
            dma((4,)),
            dma((4,)),
            dma((16,)),
            dma((16,)),
            dma((6,)),
            dma((6,)),
        ],
        compiler_params=pltpu.CompilerParams(
            collective_id=0, has_side_effects=True, vmem_limit_bytes=60 * 1024 * 1024
        ),
    )(
        tokens,
        input_norm_scale.reshape(1, D),
        outer_gate_weight,
        inner_gate_weight,
        value_weight_matrix,
        output_gate_weight,
        state_input_weight,
        write_key_weight,
        read_key_weight,
        step_size_weight.T,
        gated_conv_weight,
        input_conv_weight,
        write_conv_weight,
        read_conv_weight,
        step_size_bias,
        log_decay_rate,
        decay_spikes,
        direct_path_weight,
        head_norm_scale.reshape(1, W),
        conv_output_weight,
        state_output_weight,
    )


def solution(mesh):
    torus = Mesh(mesh.devices.reshape(NZ, NX, NC, mesh.shape["tp"]), SP_TP)
    return jax.shard_map(
        per_device,
        mesh=torus,
        in_specs=(
            P(SP_TP, None),
            P(),
            P(SP, "tp"),
            P(SP, "tp"),
            P(SP, "tp"),
            P(SP, "tp"),
            P(SP, "tp"),
            P(SP, "tp"),
            P(SP, "tp"),
            P(None, "tp"),
            P(None, "tp"),
            P(None, "tp"),
            P(None, "tp"),
            P(None, "tp"),
            P("tp"),
            P("tp"),
            P("tp", SP),
            P("tp"),
            P("tp"),
            P("tp", SP),
            P("tp", SP),
        ),
        out_specs=P(SP_TP, None),
        check_vma=False,
    )
```

```python
import functools

import jax
import jax.numpy as jnp
from jax import lax
from jax.experimental import pallas as pl
from jax.experimental.pallas import tpu as pltpu
from jax.sharding import Mesh
from jax.sharding import PartitionSpec as P

SP = ("sp_0", "sp_1", "sp_2")
SP_TP = ("sp_0", "sp_1", "sp_2", "tp")
NZ, NX, NC, NY = 16, 4, 2, 4
PLANE = NX * NC
D = 2048
ROWS = 16
W = 256
STATE = 128
HEADS = 4
HEAD_DIM = 64
OWN = 128
LEN = 512
RIM = 16
L = 128
BLOCKS = LEN // L
NA = 5
GROUPS = 8
OUTER, INNER, VALUE, CONV_T, STATE_T, OUT_GATE, STATE_IN, KEYS = range(8)
EPS = 1e-05
MESH = pl.DeviceIdType.MESH
F32 = jnp.float32
BF16 = jnp.bfloat16
HIGH = lax.Precision.HIGHEST


def silu(v):
    return v / (1.0 + jnp.exp(-v))


def dot_nn(a, b, precision=None):
    return lax.dot_general(
        a, b, (((1,), (0,)), ((), ())), precision=precision, preferred_element_type=F32
    )


def dot_nt(a, b, precision=None):
    return lax.dot_general(
        a, b, (((1,), (1,)), ((), ())), precision=precision, preferred_element_type=F32
    )


def dot_tn(a, b, precision=None):
    return lax.dot_general(
        a, b, (((0,), (0,)), ((), ())), precision=precision, preferred_element_type=F32
    )


def iota(shape, dim):
    return lax.broadcasted_iota(jnp.int32, shape, dim)


def layer_kernel(
    tok_hbm,
    scale_hbm,
    outer_w,
    inner_w,
    value_w,
    out_gate_w,
    state_in_w,
    write_w,
    read_w,
    step_w_hbm,
    gated_taps_hbm,
    input_taps_hbm,
    write_taps_hbm,
    read_taps_hbm,
    bias_hbm,
    rate_hbm,
    spikes_hbm,
    direct_hbm,
    head_scale_hbm,
    conv_out_w,
    state_out_w,
    out,
    tok,
    scale,
    step_w,
    gated_taps,
    input_taps,
    write_taps,
    read_taps,
    bias,
    rate,
    spikes,
    direct,
    head_scale,
    in_s,
    conv_part,
    before_log,
    wbuf,
    nb,
    pj,
    product,
    mixer,
    xin,
    wk,
    rk,
    within,
    cumx,
    before,
    decay,
    s_own,
    s1,
    pref,
    s2_own,
    s2,
    zin,
    s3_own,
    s3,
    t_own,
    t_plane,
    tz_own,
    t_z,
    rs_far,
    rs_right,
    rs_left,
    got_far_l,
    got_far_r,
    got_left,
    got_right,
    tok_s,
    tok_r,
    az_s,
    azl_r,
    azr_r,
    ax_s,
    axl_r,
    axr_r,
    axfl_r,
    axfr_r,
    bx_s,
    bx_r,
    bz_s,
    bzl_r,
    bzr_r,
    dd_s,
    dd_r,
    rim_s,
    rim_r,
    st_s,
    st_r,
    s2_s,
    s2_r,
    rs_s,
    rs_r,
):
    z = lax.axis_index("sp_0")
    x = lax.axis_index("sp_1")
    c = lax.axis_index("sp_2")
    y = lax.axis_index("tp")
    p = x * NC + c
    sp = z * PLANE + p

    def zm(k):
        return lax.rem(z + (k + NZ), NZ)

    def xm(k):
        return lax.rem(x + (k + NX), NX)

    def ym(k):
        return lax.rem(y + (k + NY), NY)

    def in_plane(k):
        q = lax.rem(p + k, PLANE)
        return q, (z, q // NC, lax.rem(q, NC), y)

    z_right, z_left = (zm(1), x, c, y), (zm(-1), x, c, y)
    x_right, x_left = (z, xm(1), c, y), (z, xm(-1), c, y)
    y_right, y_left = (z, x, c, ym(1)), (z, x, c, ym(-1))
    partner = (z, x, 1 - c, y)

    def along(k):
        q = lax.rem(sp + (k + NZ * PLANE), NZ * PLANE)
        r = lax.rem(q, PLANE)
        return (q // PLANE, r // NC, lax.rem(r, NC), y)

    weight_copies = [
        pltpu.make_async_copy(ref, wbuf.at[group, z, x, c], in_s.at[group])
        for group, ref in (
            (OUTER, outer_w),
            (INNER, inner_w),
            (VALUE, value_w),
            (CONV_T, conv_out_w),
            (STATE_T, state_out_w),
            (OUT_GATE, out_gate_w),
            (STATE_IN, state_in_w),
        )
    ] + [
        pltpu.make_async_copy(write_w, wbuf.at[KEYS, z, x, c, :, pl.ds(0, STATE)], in_s.at[7]),
        pltpu.make_async_copy(read_w, wbuf.at[KEYS, z, x, c, :, pl.ds(STATE, STATE)], in_s.at[8]),
    ]
    token_copies = [
        pltpu.make_async_copy(tok_hbm, tok, in_s.at[9]),
        pltpu.make_async_copy(scale_hbm, scale, in_s.at[10]),
    ]
    small_copies = [
        pltpu.make_async_copy(src, dst, in_s.at[11 + i])
        for i, (src, dst) in enumerate(
            (
                (step_w_hbm, step_w),
                (gated_taps_hbm, gated_taps),
                (input_taps_hbm, input_taps),
                (write_taps_hbm, write_taps),
                (read_taps_hbm, read_taps),
                (bias_hbm, bias),
                (rate_hbm, rate),
                (spikes_hbm, spikes),
                (direct_hbm, direct),
                (head_scale_hbm, head_scale),
            )
        )
    ]
    for copy in weight_copies + token_copies + small_copies:
        copy.start()

    barrier = pltpu.get_barrier_semaphore()

    def hello(where):
        pl.semaphore_signal(barrier, inc=1, device_id=where, device_id_type=MESH)

    hello(y_right)
    hello(y_left)
    hello(along(-1))

    def hello_plane(k, carry):
        hello(in_plane(k)[1])
        return carry

    def hello_z(k, carry):
        hello((lax.rem(z + k, NZ), x, c, y))
        return carry

    lax.fori_loop(1, PLANE, hello_plane, 0)
    lax.fori_loop(1, NZ, hello_z, 0)

    def send(src, dst, s_sem, r_sem, where):
        pltpu.make_async_remote_copy(
            src_ref=src,
            dst_ref=dst,
            send_sem=s_sem,
            recv_sem=r_sem,
            device_id=where,
            device_id_type=MESH,
        ).start()

    def wait(ref, sem):
        pltpu.make_async_copy(ref, ref, sem).wait()

    HALF = OWN // 2

    def tok_piece(k, half):
        start = pl.multiple_of(RIM + ym(k) * OWN + half * HALF, RIM)
        return nb.at[pl.ds(start, HALF)]

    def send_tok(k, half, index, where):
        piece = tok_piece(k, half)
        send(piece, piece, tok_s.at[index], tok_r.at[index], where)

    def a_block(zz, xx):
        return wbuf.at[pl.ds(0, NA), zz, xx, c]

    def a_half(zz, xx, half):
        return wbuf.at[pl.ds(0, NA), zz, xx, c, :, pl.ds(half * 128, 128)]

    def b_block(xx):
        return wbuf.at[pl.ds(NA, GROUPS - NA), z, xx, c]

    def b_chunk(group, zz):
        return wbuf.at[group, zz, :, c]

    def az_send(k_right, k_left, step):
        if step <= 7:
            blk = a_block(zm(k_right), x)
            send(blk, blk, az_s, azl_r.at[step], z_right)
        if step <= 6:
            blk = a_block(zm(k_left), x)
            send(blk, blk, az_s, azr_r.at[step], z_left)

    def offsets(s):
        if s == 0:
            return [(0, 0)]
        found = [(-s, 0)]
        if s <= 7:
            found.append((s, 1))
        return found

    def ax_send(s):
        for k, side in offsets(s):
            i = 2 * s + side
            blk = a_block(zm(k), x)
            send(blk, blk, ax_s, axl_r.at[i], x_right)
            send(blk, blk, ax_s, axr_r.at[i], x_left)

    def ax_forward(s):
        for k, side in offsets(s):
            i = 2 * s + side
            wait(a_block(zm(k), xm(-1)), axl_r.at[i])
            half = a_half(zm(k), xm(-1), 0)
            send(half, half, ax_s, axfl_r.at[i], x_right)
            wait(a_block(zm(k), xm(1)), axr_r.at[i])
            half = a_half(zm(k), xm(1), 1)
            send(half, half, ax_s, axfr_r.at[i], x_left)

    def a_across(s):
        for k, side in offsets(s):
            i = 2 * s + side
            wait(a_half(zm(k), xm(2), 0), axfl_r.at[i])
            wait(a_half(zm(k), xm(2), 1), axfr_r.at[i])
            blk = wbuf.at[pl.ds(0, NA), zm(k), :, c]
            send(blk, blk, dd_s.at[0], dd_r.at[0], partner)

    def bz_send(k_right, k_left, step, group):
        b = group - NA
        if step <= 7:
            blk = b_chunk(group, zm(k_right))
            send(blk, blk, bz_s, bzl_r.at[b * 8 + step], z_right)
        if step <= 6:
            blk = b_chunk(group, zm(k_left))
            send(blk, blk, bz_s, bzr_r.at[b * 8 + step], z_left)

    def b_across(group, k):
        blk = b_chunk(group, zm(k))
        send(blk, blk, dd_s.at[1 + group - NA], dd_r.at[1 + group - NA], partner)

    order_b = (KEYS, STATE_IN, OUT_GATE)

    def b_round(s):
        for group in order_b:
            b = group - NA
            wait(b_chunk(group, zm(-s)), bzl_r.at[b * 8 + s - 1])
            if s <= 7:
                wait(b_chunk(group, zm(s)), bzr_r.at[b * 8 + s - 1])
            bz_send(-s, s, s, group)

    def b_round_across(s):
        for group in order_b:
            b_across(group, -s)
            if 1 <= s <= 7:
                b_across(group, s)

    pl.semaphore_wait(barrier, 2 + 1 + (PLANE - 1) + (NZ - 1))
    for copy in weight_copies:
        copy.wait()
    az_send(0, 0, 0)
    for k in (1, 3, 2):
        send(b_block(x), b_block(x), bx_s.at[k], bx_r.at[k], (z, xm(k), c, y))
    ax_send(0)

    for copy in token_copies:
        copy.wait()
    token_rows = tok[...].astype(F32)
    scaled = token_rows * lax.rsqrt(
        jnp.mean(token_rows * token_rows, axis=1, keepdims=True) + EPS
    )
    own_row = pl.multiple_of(RIM + y * OWN, RIM)
    nb[pl.ds(own_row, OWN)] = (scaled * scale[...].astype(F32).reshape(1, D)).astype(BF16)
    send_tok(0, 0, 0, y_right)
    send_tok(0, 1, 1, y_left)
    send_tok(0, 1, 2, y_right)
    send_tok(0, 0, 3, y_left)

    for s in range(1, 10):
        if s <= 8:
            wait(a_block(zm(-s), x), azl_r.at[s - 1])
            if s <= 7:
                wait(a_block(zm(s), x), azr_r.at[s - 1])
            az_send(-s, s, s)
            ax_send(s)
        if s == 1:
            for k in (1, 3, 2):
                wait(b_block(xm(-k)), bx_r.at[k])
            for group in order_b:
                bz_send(0, 0, 0, group)
        else:
            b_round(s - 1)
        if s >= 2:
            ax_forward(s - 2)
            b_round_across(s - 2)
        if s >= 4:
            a_across(s - 4)
        if s == 3:
            wait(tok_piece(-1, 0), tok_r.at[0])
            send_tok(-1, 0, 4, y_right)
            wait(tok_piece(1, 1), tok_r.at[1])
            send_tok(1, 1, 5, y_left)
    b_round_across(8)
    a_across(6)
    ax_forward(8)

    wait(tok_piece(-1, 1), tok_r.at[2])
    wait(tok_piece(1, 0), tok_r.at[3])
    wait(tok_piece(2, 0), tok_r.at[4])
    wait(tok_piece(2, 1), tok_r.at[5])

    @pl.when(sp < NZ * PLANE - 1)
    def _():
        send(nb.at[pl.ds(LEN, RIM)], nb.at[pl.ds(0, RIM)], rim_s, rim_r, along(1))

    @pl.when(sp == 0)
    def _():
        nb[0:RIM] = jnp.zeros((RIM, D), BF16)

    for copy in small_copies:
        copy.wait()

    step_raw = dot_nt(step_w[...], nb[RIM : RIM + LEN])
    head_row = iota((HEADS, LEN), 0)

    def per_head(ref, index):
        return functools.reduce(
            lambda got, h: jnp.where(index == h, ref[h], got),
            range(1, HEADS),
            jnp.full(index.shape, ref[0], F32),
        )

    shifted = step_raw + per_head(bias, head_row)
    step = jnp.maximum(shifted, 0.0) + jnp.log1p(jnp.exp(-jnp.abs(shifted)))
    log_step = step * (-jnp.exp(per_head(rate, head_row))) + spikes[...]
    ramp = (iota((L, L), 0) <= iota((L, L), 1)).astype(F32)
    spread = (iota((HEADS, W), 1) // HEAD_DIM == iota((HEADS, W), 0)).astype(F32)
    total = jnp.zeros((1, W), F32)
    cum_rows = []
    for b in range(BLOCKS):
        rows = dot_nn(log_step[:, b * L : (b + 1) * L], ramp, HIGH)
        cum_rows.append(rows)
        wide = dot_tn(rows, spread, HIGH)
        cumx[b] = wide
        decay[b] = wide[L - 1 : L]
        before_log[b] = total
        total = total + wide[L - 1 : L]
    t_own[0] = total

    for k in range(1, PLANE):
        _, where = in_plane(k)
        send(t_own, t_plane.at[pl.ds(p, 1)], st_s.at[0], st_r.at[0], where)
    t_plane[p] = total

    a_across(7)

    @pl.when(sp > 0)
    def _():
        wait(nb.at[pl.ds(0, RIM)], rim_r)

    for group in (STATE_IN, KEYS):
        wait(wbuf.at[group, :, :, 1 - c], dd_r.at[1 + group - NA])

    def project(group, carry):
        acc = dot_nn(nb[...], wbuf[group].reshape(D, W))
        pj[group] = acc.astype(BF16).astype(F32)
        return carry

    lax.fori_loop(STATE_IN, KEYS + 1, project, 0)
    a_across(8)

    def causal(ref, taps, first, last):
        count = taps.shape[0]
        weights = taps[...].astype(F32)
        start = RIM - count + 1
        running = weights[0:1] * ref[start : start + LEN, first:last]
        for k in range(1, count):
            running = running + weights[k : k + 1] * ref[start + k : start + k + LEN, first:last]
        return running

    xin[...] = silu(causal(pj.at[STATE_IN], input_taps, 0, W))
    wk[...] = silu(causal(pj.at[KEYS], write_taps, 0, STATE)).astype(BF16)
    rk[...] = silu(causal(pj.at[KEYS], read_taps, STATE, W)).astype(BF16)

    state = jnp.zeros((STATE, W), F32)
    lane_head = iota((L, W), 1) // HEAD_DIM
    spread_l = (iota((HEADS, HEADS * L), 1) // L == iota((HEADS, HEADS * L), 0)).astype(F32)
    keep = iota((L, HEADS * L), 0) >= lax.rem(iota((L, HEADS * L), 1), L)
    weighted = []
    for b in range(BLOCKS):
        steps = dot_tn(step[:, b * L : (b + 1) * L], spread, HIGH)
        heavy = xin[b * L : (b + 1) * L] * steps
        weighted.append(heavy.astype(BF16))
        to_end = jnp.exp(decay[b] - cumx[b])
        own = dot_tn(wk[b * L : (b + 1) * L], (heavy * to_end).astype(BF16))
        before[b] = state
        state = state * jnp.exp(decay[b]) + own
    s_own[...] = state.astype(BF16).reshape(PLANE, ROWS, W)
    for k in range(1, PLANE):
        q, where = in_plane(k)
        send(s_own.at[q], s1.at[p], st_s.at[2], st_r.at[2], where)
    s1[p] = s_own[p]

    wait(t_plane.at[pl.ds(0, PLANE - 1)], st_r.at[0])
    tz_own[0] = jnp.sum(t_plane[...], axis=0)

    def send_tz(k, carry):
        there = lax.rem(z + k, NZ)
        send(tz_own, t_z.at[pl.ds(z, 1)], st_s.at[1], st_r.at[1], (there, x, c, y))
        return carry

    lax.fori_loop(1, NZ, send_tz, 0)

    def within_block(b):
        rows = slice(b * L, (b + 1) * L)
        scores = dot_nt(rk[rows], wk[rows])
        cols = dot_tn(cum_rows[b], spread_l, HIGH)
        flat = jnp.concatenate([cum_rows[b][h : h + 1] for h in range(HEADS)], axis=1)
        damping = jnp.exp(jnp.where(keep, cols - flat, -jnp.inf))
        mixed = (jnp.concatenate([scores] * HEADS, axis=1) * damping).astype(BF16)
        stacked = jnp.concatenate(
            [jnp.where(lane_head == h, weighted[b], jnp.zeros_like(weighted[b])) for h in range(HEADS)],
            axis=0,
        )
        within[rows] = dot_nn(mixed, stacked)

    for b in range(BLOCKS):
        within_block(b)

    wait(s1.at[pl.ds(0, PLANE - 1)], st_r.at[2])
    running = jnp.zeros((ROWS, W), F32)
    for i in range(PLANE):
        pref[i] = running
        running = running * jnp.exp(t_plane[i]) + s1[i].astype(F32)
    s2_own[...] = running.astype(BF16)

    def send_s2(k, carry):
        @pl.when(z + k < NZ)
        def _():
            send(s2_own, s2.at[z], s2_s.at[k], s2_r.at[z], (z + k, x, c, y))

        return carry

    lax.fori_loop(1, NZ, send_s2, 0)

    wait(wbuf.at[OUT_GATE, :, :, 1 - c], dd_r.at[1 + OUT_GATE - NA])
    wait(wbuf.at[pl.ds(0, NA), :, :, 1 - c], dd_r.at[0])
    lax.fori_loop(OUTER, VALUE + 1, project, 0)
    lax.fori_loop(OUT_GATE, OUT_GATE + 1, project, 0)
    product[...] = pj[INNER] * pj[VALUE]
    mixer[...] = (pj[OUTER, RIM : RIM + LEN] * causal(product, gated_taps, 0, W)).astype(BF16)

    def conv_block(b, carry):
        start = pl.multiple_of(b * OWN, OWN)
        conv_part[pl.ds(start, OWN)] = dot_nt(
            mixer[pl.ds(start, OWN)], wbuf[CONV_T].reshape(D, W)
        )
        return carry

    lax.fori_loop(0, NY, conv_block, 0)

    wait(t_z.at[pl.ds(0, NZ - 1)], st_r.at[1])
    zin[...] = jnp.zeros((ROWS, W), F32)

    def take_s2(k, carry):
        @pl.when(k < z)
        def _():
            wait(s2.at[k], s2_r.at[k])
            zin[...] = zin[...] * jnp.exp(t_z[k]) + s2[k].astype(F32)

        return carry

    lax.fori_loop(0, NZ - 1, take_s2, 0)
    arriving = zin[...]
    logs = jnp.zeros((1, W), F32)
    for i in range(PLANE):
        s3_own[i] = (pref[i] + arriving * jnp.exp(logs)).astype(BF16)
        logs = logs + t_plane[i]
    for k in range(1, PLANE):
        q, where = in_plane(k)
        send(s3_own.at[q], s3.at[p], st_s.at[3], st_r.at[3], where)
    s3[p] = s3_own[p]

    lane = iota((1, W), 1) // HEAD_DIM
    direct_row = per_head(direct, lane)
    same_head = (iota((W, W), 0) // HEAD_DIM == iota((W, W), 1) // HEAD_DIM).astype(F32) * (
        1.0 / HEAD_DIM
    )
    gate = silu(pj[OUT_GATE, RIM : RIM + LEN])
    pj[OUT_GATE, RIM : RIM + LEN] = gate

    wait(s3.at[pl.ds(0, PLANE - 1)], st_r.at[3])
    entering = s3[...].reshape(STATE, W).astype(F32)

    def partial(k):
        b = ym(k)
        rows = pl.ds(pl.multiple_of(b * L, L), L)
        enter = (before[b] + jnp.exp(before_log[b]) * entering).astype(BF16)
        head_out = (
            within[rows]
            + dot_nn(rk[rows], enter) * jnp.exp(cumx[b])
            + direct_row * xin[rows]
        )
        gated = head_out * pj[OUT_GATE, pl.ds(pl.multiple_of(RIM + b * L, RIM), L)]
        mean = dot_nn(gated * gated, same_head, HIGH)
        part = (gated * lax.rsqrt(mean + EPS) * head_scale[...].astype(F32).reshape(1, W)).astype(BF16)
        return conv_part[rows] + dot_nt(part, wbuf[STATE_T].reshape(D, W))

    rs_far[...] = partial(2).astype(BF16)
    send(rs_far.at[0:HALF], got_far_l, rs_s.at[0], rs_r.at[0], y_right)
    send(rs_far.at[HALF:OWN], got_far_r, rs_s.at[1], rs_r.at[1], y_left)
    to_right = partial(1)
    rs_right[HALF:OWN] = to_right[HALF:OWN].astype(BF16)
    send(rs_right.at[HALF:OWN], got_left.at[HALF:OWN], rs_s.at[2], rs_r.at[2], y_right)
    to_left = partial(-1)
    rs_left[0:HALF] = to_left[0:HALF].astype(BF16)
    send(rs_left.at[0:HALF], got_right.at[0:HALF], rs_s.at[3], rs_r.at[3], y_left)
    wait(got_far_l, rs_r.at[0])
    rs_right[0:HALF] = (to_right[0:HALF] + got_far_l[...].astype(F32)).astype(BF16)
    send(rs_right.at[0:HALF], got_left.at[0:HALF], rs_s.at[4], rs_r.at[4], y_right)
    wait(got_far_r, rs_r.at[1])
    rs_left[HALF:OWN] = (to_left[HALF:OWN] + got_far_r[...].astype(F32)).astype(BF16)
    send(rs_left.at[HALF:OWN], got_right.at[HALF:OWN], rs_s.at[5], rs_r.at[5], y_left)
    mine = partial(0)

    for index, half in ((0, 0), (1, 1), (2, 1), (3, 0)):
        wait(tok_piece(0, half), tok_s.at[index])
    wait(tok_piece(-1, 0), tok_s.at[4])
    wait(tok_piece(1, 1), tok_s.at[5])
    wait(wbuf.at[pl.ds(0, NA), pl.ds(0, NZ - 1), 0, 0], az_s)
    wait(wbuf.at[pl.ds(0, NA), :, pl.ds(0, 3), 0], ax_s)
    for k in (1, 2, 3):
        wait(b_block(x), bx_s.at[k])
    wait(wbuf.at[pl.ds(NA, GROUPS - NA), pl.ds(0, NZ - 1), :, 0], bz_s)
    wait(wbuf.at[pl.ds(0, NA), :, :, c], dd_s.at[0])
    for b in range(GROUPS - NA):
        wait(wbuf.at[NA + b, :, :, c], dd_s.at[1 + b])

    @pl.when(sp < NZ * PLANE - 1)
    def _():
        wait(nb.at[pl.ds(LEN, RIM)], rim_s)

    wait(t_plane.at[pl.ds(0, PLANE - 1)], st_s.at[0])
    wait(t_z.at[pl.ds(0, NZ - 1)], st_s.at[1])
    wait(s_own.at[pl.ds(0, PLANE - 1)], st_s.at[2])
    wait(s3_own.at[pl.ds(0, PLANE - 1)], st_s.at[3])

    def left_s2(k, carry):
        @pl.when(z + k < NZ)
        def _():
            wait(s2_own, s2_s.at[k])

        return carry

    lax.fori_loop(1, NZ, left_s2, 0)
    wait(rs_far.at[0:HALF], rs_s.at[0])
    wait(rs_far.at[HALF:OWN], rs_s.at[1])
    wait(rs_right.at[HALF:OWN], rs_s.at[2])
    wait(rs_left.at[0:HALF], rs_s.at[3])
    wait(rs_right.at[0:HALF], rs_s.at[4])
    wait(rs_left.at[HALF:OWN], rs_s.at[5])

    wait(got_left.at[HALF:OWN], rs_r.at[2])
    wait(got_right.at[0:HALF], rs_r.at[3])
    wait(got_left.at[0:HALF], rs_r.at[4])
    wait(got_right.at[HALF:OWN], rs_r.at[5])
    out[...] = (mine + got_left[...].astype(F32) + got_right[...].astype(F32)).astype(BF16)


def per_device(
    tokens,
    input_norm_scale,
    outer_gate_weight,
    inner_gate_weight,
    value_weight_matrix,
    output_gate_weight,
    state_input_weight,
    write_key_weight,
    read_key_weight,
    step_size_weight,
    gated_conv_weight,
    input_conv_weight,
    write_conv_weight,
    read_conv_weight,
    step_size_bias,
    log_decay_rate,
    decay_spikes,
    direct_path_weight,
    head_norm_scale,
    conv_output_weight,
    state_output_weight,
):
    vmem = pl.BlockSpec(memory_space=pltpu.VMEM)
    dma = pltpu.SemaphoreType.DMA
    return pl.pallas_call(
        layer_kernel,
        out_shape=jax.ShapeDtypeStruct((OWN, D), BF16),
        in_specs=[pl.BlockSpec(memory_space=pl.ANY)] * 21,
        out_specs=vmem,
        scratch_shapes=[
            pltpu.VMEM((OWN, D), BF16),
            pltpu.VMEM((D,), BF16),
            pltpu.VMEM((HEADS, D), BF16),
            pltpu.VMEM((3, W), BF16),
            pltpu.VMEM((4, W), BF16),
            pltpu.VMEM((4, STATE), BF16),
            pltpu.VMEM((4, STATE), BF16),
            pltpu.SMEM((HEADS,), F32),
            pltpu.SMEM((HEADS,), F32),
            pltpu.VMEM((HEADS, LEN), F32),
            pltpu.SMEM((HEADS,), F32),
            pltpu.VMEM((W,), BF16),
            dma((21,)),
            pltpu.VMEM((LEN, D), F32),
            pltpu.VMEM((BLOCKS, 1, W), F32),
            pltpu.VMEM((GROUPS, NZ, NX, NC, ROWS, W), BF16),
            pltpu.VMEM((RIM + LEN, D), BF16),
            pltpu.VMEM((GROUPS, RIM + LEN, W), F32),
            pltpu.VMEM((RIM + LEN, W), F32),
            pltpu.VMEM((LEN, W), BF16),
            pltpu.VMEM((LEN, W), F32),
            pltpu.VMEM((LEN, STATE), BF16),
            pltpu.VMEM((LEN, STATE), BF16),
            pltpu.VMEM((LEN, W), F32),
            pltpu.VMEM((BLOCKS, L, W), F32),
            pltpu.VMEM((BLOCKS, STATE, W), F32),
            pltpu.VMEM((BLOCKS, 1, W), F32),
            pltpu.VMEM((PLANE, ROWS, W), BF16),
            pltpu.VMEM((PLANE, ROWS, W), BF16),
            pltpu.VMEM((PLANE, ROWS, W), F32),
            pltpu.VMEM((ROWS, W), BF16),
            pltpu.VMEM((NZ, ROWS, W), BF16),
            pltpu.VMEM((ROWS, W), F32),
            pltpu.VMEM((PLANE, ROWS, W), BF16),
            pltpu.VMEM((PLANE, ROWS, W), BF16),
            pltpu.VMEM((1, 1, W), F32),
            pltpu.VMEM((PLANE, 1, W), F32),
            pltpu.VMEM((1, 1, W), F32),
            pltpu.VMEM((NZ, 1, W), F32),
            pltpu.VMEM((OWN, D), BF16),
            pltpu.VMEM((OWN, D), BF16),
            pltpu.VMEM((OWN, D), BF16),
            pltpu.VMEM((OWN // 2, D), BF16),
            pltpu.VMEM((OWN // 2, D), BF16),
            pltpu.VMEM((OWN, D), BF16),
            pltpu.VMEM((OWN, D), BF16),
            dma((6,)),
            dma((6,)),
            dma,
            dma((8,)),
            dma((8,)),
            dma,
            dma((18,)),
            dma((18,)),
            dma((18,)),
            dma((18,)),
            dma((4,)),
            dma((4,)),
            dma,
            dma((24,)),
            dma((24,)),
            dma((4,)),
            dma((4,)),
            dma,
            dma,
            dma((4,)),
            dma((4,)),
            dma((16,)),
            dma((16,)),
            dma((6,)),
            dma((6,)),
        ],
        compiler_params=pltpu.CompilerParams(
            collective_id=0, has_side_effects=True, vmem_limit_bytes=60 * 1024 * 1024
        ),
    )(
        tokens,
        input_norm_scale,
        outer_gate_weight,
        inner_gate_weight,
        value_weight_matrix,
        output_gate_weight,
        state_input_weight,
        write_key_weight,
        read_key_weight,
        step_size_weight.T,
        gated_conv_weight,
        input_conv_weight,
        write_conv_weight,
        read_conv_weight,
        step_size_bias,
        log_decay_rate,
        decay_spikes,
        direct_path_weight,
        head_norm_scale,
        conv_output_weight.T,
        state_output_weight.T,
    )


def solution(mesh):
    torus = Mesh(mesh.devices.reshape(NZ, NX, NC, mesh.shape["tp"]), SP_TP)
    return jax.shard_map(
        per_device,
        mesh=torus,
        in_specs=(
            P(SP_TP, None),
            P(),
            P(SP, "tp"),
            P(SP, "tp"),
            P(SP, "tp"),
            P(SP, "tp"),
            P(SP, "tp"),
            P(SP, "tp"),
            P(SP, "tp"),
            P(None, "tp"),
            P(None, "tp"),
            P(None, "tp"),
            P(None, "tp"),
            P(None, "tp"),
            P("tp"),
            P("tp"),
            P("tp", SP),
            P("tp"),
            P("tp"),
            P("tp", SP),
            P("tp", SP),
        ),
        out_specs=P(SP_TP, None),
        check_vma=False,
    )
```

```python
import functools

import jax
import jax.numpy as jnp
from jax import lax
from jax.experimental import pallas as pl
from jax.experimental.pallas import tpu as pltpu
from jax.sharding import Mesh
from jax.sharding import PartitionSpec as P

SP = ("sp_0", "sp_1", "sp_2")
SP_TP = ("sp_0", "sp_1", "sp_2", "tp")
NZ, NX, NC, NY = 16, 4, 2, 4
PLANE = NX * NC
D = 2048
ROWS = 16
W = 256
STATE = 128
HEADS = 4
HEAD_DIM = 64
OWN = 128
LEN = 512
RIM = 16
L = 128
BLOCKS = LEN // L
NA = 5
GROUPS = 8
OUTER, INNER, VALUE, CONV_T, STATE_T, OUT_GATE, STATE_IN, KEYS = range(8)
EPS = 1e-05
MESH = pl.DeviceIdType.MESH
F32 = jnp.float32
BF16 = jnp.bfloat16
HIGH = lax.Precision.HIGHEST


def silu(v):
    return v / (1.0 + jnp.exp(-v))


def dot_nn(a, b, precision=None):
    return lax.dot_general(
        a, b, (((1,), (0,)), ((), ())), precision=precision, preferred_element_type=F32
    )


def dot_nt(a, b, precision=None):
    return lax.dot_general(
        a, b, (((1,), (1,)), ((), ())), precision=precision, preferred_element_type=F32
    )


def dot_tn(a, b, precision=None):
    return lax.dot_general(
        a, b, (((0,), (0,)), ((), ())), precision=precision, preferred_element_type=F32
    )


def iota(shape, dim):
    return lax.broadcasted_iota(jnp.int32, shape, dim)


def layer_kernel(
    tok_hbm,
    scale_hbm,
    outer_w,
    inner_w,
    value_w,
    out_gate_w,
    state_in_w,
    write_w,
    read_w,
    step_w_hbm,
    gated_taps_hbm,
    input_taps_hbm,
    write_taps_hbm,
    read_taps_hbm,
    bias_hbm,
    rate_hbm,
    spikes_hbm,
    direct_hbm,
    head_scale_hbm,
    conv_out_w,
    state_out_w,
    out,
    tok,
    scale,
    step_w,
    gated_taps,
    input_taps,
    write_taps,
    read_taps,
    bias,
    rate,
    spikes,
    direct,
    head_scale,
    in_s,
    handed,
    conv_part,
    before_log,
    wbuf,
    nb,
    pj,
    product,
    mixer,
    xin,
    wk,
    rk,
    within,
    cumx,
    before,
    decay,
    s_own,
    s1,
    pref,
    s2_own,
    s2,
    zin,
    s3_own,
    s3,
    t_own,
    t_plane,
    tz_own,
    t_z,
    rs_far,
    rs_right,
    rs_left,
    got_far_l,
    got_far_r,
    got_left,
    got_right,
    tok_s,
    tok_r,
    az_s,
    azl_r,
    azr_r,
    ax_s,
    axl_r,
    axr_r,
    axfl_r,
    axfr_r,
    bx_s,
    bx_r,
    bz_s,
    bzl_r,
    bzr_r,
    pair_s,
    pair_r,
    dd_s,
    dd_r,
    rim_s,
    rim_r,
    st_s,
    st_r,
    s2_s,
    s2_r,
    rs_s,
    rs_r,
):
    z = lax.axis_index("sp_0")
    x = lax.axis_index("sp_1")
    c = lax.axis_index("sp_2")
    y = lax.axis_index("tp")
    p = x * NC + c
    sp = z * PLANE + p

    def zm(k):
        return lax.rem(z + (k + NZ), NZ)

    def xm(k):
        return lax.rem(x + (k + NX), NX)

    def ym(k):
        return lax.rem(y + (k + NY), NY)

    def in_plane(k):
        q = lax.rem(p + k, PLANE)
        return q, (z, q // NC, lax.rem(q, NC), y)

    z_right, z_left = (zm(1), x, c, y), (zm(-1), x, c, y)
    x_right, x_left = (z, xm(1), c, y), (z, xm(-1), c, y)
    y_right, y_left = (z, x, c, ym(1)), (z, x, c, ym(-1))
    partner = (z, x, 1 - c, y)

    def along(k):
        q = lax.rem(sp + (k + NZ * PLANE), NZ * PLANE)
        r = lax.rem(q, PLANE)
        return (q // PLANE, r // NC, lax.rem(r, NC), y)

    def weight_copies(whole):
        return [
            pltpu.make_async_copy(ref, whole.at[group], in_s.at[group])
            for group, ref in (
                (OUTER, outer_w),
                (INNER, inner_w),
                (VALUE, value_w),
                (CONV_T, conv_out_w),
                (STATE_T, state_out_w),
                (OUT_GATE, out_gate_w),
                (STATE_IN, state_in_w),
            )
        ] + [
            pltpu.make_async_copy(write_w, whole.at[KEYS, :, pl.ds(0, STATE)], in_s.at[7]),
            pltpu.make_async_copy(read_w, whole.at[KEYS, :, pl.ds(STATE, STATE)], in_s.at[8]),
        ]

    in_place = wbuf.at[:, z, x, 0]
    token_copies = [
        pltpu.make_async_copy(tok_hbm, tok, in_s.at[9]),
        pltpu.make_async_copy(scale_hbm, scale, in_s.at[10]),
    ]
    small_copies = [
        pltpu.make_async_copy(src, dst, in_s.at[11 + i])
        for i, (src, dst) in enumerate(
            (
                (step_w_hbm, step_w),
                (gated_taps_hbm, gated_taps),
                (input_taps_hbm, input_taps),
                (write_taps_hbm, write_taps),
                (read_taps_hbm, read_taps),
                (bias_hbm, bias),
                (rate_hbm, rate),
                (spikes_hbm, spikes),
                (direct_hbm, direct),
                (head_scale_hbm, head_scale),
            )
        )
    ]

    @pl.when(c == 0)
    def _():
        for copy in weight_copies(in_place):
            copy.start()

    @pl.when(c == 1)
    def _():
        for copy in weight_copies(handed):
            copy.start()

    for copy in token_copies + small_copies:
        copy.start()

    barrier = pltpu.get_barrier_semaphore()

    def hello(where):
        pl.semaphore_signal(barrier, inc=1, device_id=where, device_id_type=MESH)

    hello(y_right)
    hello(y_left)
    hello(along(-1))

    hello(partner)

    @pl.when(c == 0)
    def _():
        for where in (z_right, z_left, x_right, x_left, (z, xm(2), c, y)):
            hello(where)

    def send(src, dst, s_sem, r_sem, where):
        pltpu.make_async_remote_copy(
            src_ref=src,
            dst_ref=dst,
            send_sem=s_sem,
            recv_sem=r_sem,
            device_id=where,
            device_id_type=MESH,
        ).start()

    def wait(ref, sem):
        pltpu.make_async_copy(ref, ref, sem).wait()

    HALF = OWN // 2

    def tok_piece(k, half):
        start = pl.multiple_of(RIM + ym(k) * OWN + half * HALF, RIM)
        return nb.at[pl.ds(start, HALF)]

    def send_tok(k, half, index, where):
        piece = tok_piece(k, half)
        send(piece, piece, tok_s.at[index], tok_r.at[index], where)

    def a_block(zz, xx):
        return wbuf.at[pl.ds(0, NA), zz, xx]

    def a_half(zz, xx, half):
        return wbuf.at[pl.ds(0, NA), zz, xx, half]

    def b_block(xx):
        return wbuf.at[pl.ds(NA, GROUPS - NA), z, xx]

    def b_chunk(group, zz):
        return wbuf.at[group, zz]

    def az_send(k_right, k_left, step):
        if step <= 7:
            blk = a_block(zm(k_right), x)
            send(blk, blk, az_s, azl_r.at[step], z_right)
        if step <= 6:
            blk = a_block(zm(k_left), x)
            send(blk, blk, az_s, azr_r.at[step], z_left)

    def offsets(s):
        if s == 0:
            return [(0, 0)]
        found = [(-s, 0)]
        if s <= 7:
            found.append((s, 1))
        return found

    def ax_send(s):
        for k, side in offsets(s):
            i = 2 * s + side
            blk = a_block(zm(k), x)
            send(blk, blk, ax_s, axl_r.at[i], x_right)
            send(blk, blk, ax_s, axr_r.at[i], x_left)

    def ax_forward(s):
        for k, side in offsets(s):
            i = 2 * s + side
            wait(a_block(zm(k), xm(-1)), axl_r.at[i])
            half = a_half(zm(k), xm(-1), 0)
            send(half, half, ax_s, axfl_r.at[i], x_right)
            wait(a_block(zm(k), xm(1)), axr_r.at[i])
            half = a_half(zm(k), xm(1), 1)
            send(half, half, ax_s, axfr_r.at[i], x_left)

    def a_across(s):
        for k, side in offsets(s):
            i = 2 * s + side
            wait(a_half(zm(k), xm(2), 0), axfl_r.at[i])
            wait(a_half(zm(k), xm(2), 1), axfr_r.at[i])
            blk = wbuf.at[pl.ds(0, NA), zm(k)]
            send(blk, blk, dd_s.at[0], dd_r.at[0], partner)

    def bz_send(k_right, k_left, step, group):
        b = group - NA
        if step <= 7:
            blk = b_chunk(group, zm(k_right))
            send(blk, blk, bz_s, bzl_r.at[b * 8 + step], z_right)
        if step <= 6:
            blk = b_chunk(group, zm(k_left))
            send(blk, blk, bz_s, bzr_r.at[b * 8 + step], z_left)

    def b_across(group, k):
        blk = b_chunk(group, zm(k))
        send(blk, blk, dd_s.at[1 + group - NA], dd_r.at[1 + group - NA], partner)

    order_b = (KEYS, STATE_IN, OUT_GATE)

    def b_round(s):
        for group in order_b:
            b = group - NA
            wait(b_chunk(group, zm(-s)), bzl_r.at[b * 8 + s - 1])
            if s <= 7:
                wait(b_chunk(group, zm(s)), bzr_r.at[b * 8 + s - 1])
            bz_send(-s, s, s, group)

    def b_round_across(s):
        for group in order_b:
            b_across(group, -s)
            if 1 <= s <= 7:
                b_across(group, s)

    @pl.when(c == 1)
    def _():
        pl.semaphore_wait(barrier, 4)
        for copy in weight_copies(handed):
            copy.wait()
        send(handed, wbuf.at[:, z, x, 1], pair_s, pair_r, partner)

    @pl.when(c == 0)
    def _():
        pl.semaphore_wait(barrier, 9)
        for copy in weight_copies(in_place):
            copy.wait()
        wait(wbuf.at[:, z, x, 1], pair_r)
        az_send(0, 0, 0)
        for k in (1, 3, 2):
            send(b_block(x), b_block(x), bx_s.at[k], bx_r.at[k], (z, xm(k), c, y))
        ax_send(0)

    for copy in token_copies:
        copy.wait()
    token_rows = tok[...].astype(F32)
    scaled = token_rows * lax.rsqrt(
        jnp.mean(token_rows * token_rows, axis=1, keepdims=True) + EPS
    )
    own_row = pl.multiple_of(RIM + y * OWN, RIM)
    nb[pl.ds(own_row, OWN)] = (scaled * scale[...].astype(F32).reshape(1, D)).astype(BF16)
    send_tok(0, 0, 0, y_right)
    send_tok(0, 1, 1, y_left)
    send_tok(0, 1, 2, y_right)
    send_tok(0, 0, 3, y_left)

    def pass_tokens():
        wait(tok_piece(-1, 0), tok_r.at[0])
        send_tok(-1, 0, 4, y_right)
        wait(tok_piece(1, 1), tok_r.at[1])
        send_tok(1, 1, 5, y_left)

    @pl.when(c == 1)
    def _():
        pass_tokens()

    @pl.when(c == 0)
    def _():
        for s in range(1, 10):
            if s <= 8:
                wait(a_block(zm(-s), x), azl_r.at[s - 1])
                if s <= 7:
                    wait(a_block(zm(s), x), azr_r.at[s - 1])
                az_send(-s, s, s)
                ax_send(s)
            if s == 1:
                for k in (1, 3, 2):
                    wait(b_block(xm(-k)), bx_r.at[k])
                for group in order_b:
                    bz_send(0, 0, 0, group)
            else:
                b_round(s - 1)
            if s >= 2:
                ax_forward(s - 2)
                b_round_across(s - 2)
            if s >= 4:
                a_across(s - 4)
            if s == 4:
                pass_tokens()
        b_round_across(8)
        a_across(6)
        ax_forward(8)

    wait(tok_piece(-1, 1), tok_r.at[2])
    wait(tok_piece(1, 0), tok_r.at[3])
    wait(tok_piece(2, 0), tok_r.at[4])
    wait(tok_piece(2, 1), tok_r.at[5])

    @pl.when(sp < NZ * PLANE - 1)
    def _():
        send(nb.at[pl.ds(LEN, RIM)], nb.at[pl.ds(0, RIM)], rim_s, rim_r, along(1))

    @pl.when(sp == 0)
    def _():
        nb[0:RIM] = jnp.zeros((RIM, D), BF16)

    for copy in small_copies:
        copy.wait()

    step_raw = dot_nt(step_w[...], nb[RIM : RIM + LEN])
    head_row = iota((HEADS, LEN), 0)

    def per_head(ref, index):
        return functools.reduce(
            lambda got, h: jnp.where(index == h, ref[h], got),
            range(1, HEADS),
            jnp.full(index.shape, ref[0], F32),
        )

    shifted = step_raw + per_head(bias, head_row)
    step = jnp.maximum(shifted, 0.0) + jnp.log1p(jnp.exp(-jnp.abs(shifted)))
    log_step = step * (-jnp.exp(per_head(rate, head_row))) + spikes[...]
    ramp = (iota((L, L), 0) <= iota((L, L), 1)).astype(F32)
    spread = (iota((HEADS, W), 1) // HEAD_DIM == iota((HEADS, W), 0)).astype(F32)
    total = jnp.zeros((1, W), F32)
    cum_rows = []
    for b in range(BLOCKS):
        rows = dot_nn(log_step[:, b * L : (b + 1) * L], ramp, HIGH)
        cum_rows.append(rows)
        wide = dot_tn(rows, spread, HIGH)
        cumx[b] = wide
        decay[b] = wide[L - 1 : L]
        before_log[b] = total
        total = total + wide[L - 1 : L]
    t_own[0] = total

    @pl.when(c == 0)
    def _():
        a_across(7)

    @pl.when(sp > 0)
    def _():
        wait(nb.at[pl.ds(0, RIM)], rim_r)

    @pl.when(c == 1)
    def _():
        for group in (STATE_IN, KEYS):
            wait(wbuf.at[group], dd_r.at[1 + group - NA])

    for k in range(1, PLANE):
        _, where = in_plane(k)
        send(t_own, t_plane.at[pl.ds(p, 1)], st_s.at[0], st_r.at[0], where)
    t_plane[p] = total


    def project(group, carry):
        acc = dot_nn(nb[...], wbuf[group].reshape(D, W))
        pj[group] = acc.astype(BF16).astype(F32)
        return carry

    lax.fori_loop(STATE_IN, KEYS + 1, project, 0)

    @pl.when(c == 0)
    def _():
        a_across(8)


    def causal(ref, taps, first, last):
        count = taps.shape[0]
        weights = taps[...].astype(F32)
        start = RIM - count + 1
        running = weights[0:1] * ref[start : start + LEN, first:last]
        for k in range(1, count):
            running = running + weights[k : k + 1] * ref[start + k : start + k + LEN, first:last]
        return running

    xin[...] = silu(causal(pj.at[STATE_IN], input_taps, 0, W))
    wk[...] = silu(causal(pj.at[KEYS], write_taps, 0, STATE)).astype(BF16)
    rk[...] = silu(causal(pj.at[KEYS], read_taps, STATE, W)).astype(BF16)

    state = jnp.zeros((STATE, W), F32)
    lane_head = iota((L, W), 1) // HEAD_DIM
    spread_l = (iota((HEADS, HEADS * L), 1) // L == iota((HEADS, HEADS * L), 0)).astype(F32)
    keep = iota((L, HEADS * L), 0) >= lax.rem(iota((L, HEADS * L), 1), L)
    weighted = []
    for b in range(BLOCKS):
        steps = dot_tn(step[:, b * L : (b + 1) * L], spread, HIGH)
        heavy = xin[b * L : (b + 1) * L] * steps
        weighted.append(heavy.astype(BF16))
        to_end = jnp.exp(decay[b] - cumx[b])
        own = dot_tn(wk[b * L : (b + 1) * L], (heavy * to_end).astype(BF16))
        before[b] = state
        state = state * jnp.exp(decay[b]) + own
    s_own[...] = state.astype(BF16).reshape(PLANE, ROWS, W)
    for k in range(1, PLANE):
        q, where = in_plane(k)
        send(s_own.at[q], s1.at[p], st_s.at[2], st_r.at[2], where)
    s1[p] = s_own[p]

    wait(t_plane.at[pl.ds(0, PLANE - 1)], st_r.at[0])
    tz_own[0] = jnp.sum(t_plane[...], axis=0)

    def send_tz(k, carry):
        there = lax.rem(z + k, NZ)
        send(tz_own, t_z.at[pl.ds(z, 1)], st_s.at[1], st_r.at[1], (there, x, c, y))
        return carry

    lax.fori_loop(1, NZ, send_tz, 0)

    def within_block(b):
        rows = slice(b * L, (b + 1) * L)
        scores = dot_nt(rk[rows], wk[rows])
        cols = dot_tn(cum_rows[b], spread_l, HIGH)
        flat = jnp.concatenate([cum_rows[b][h : h + 1] for h in range(HEADS)], axis=1)
        damping = jnp.exp(jnp.where(keep, cols - flat, -jnp.inf))
        mixed = (jnp.concatenate([scores] * HEADS, axis=1) * damping).astype(BF16)
        stacked = jnp.concatenate(
            [jnp.where(lane_head == h, weighted[b], jnp.zeros_like(weighted[b])) for h in range(HEADS)],
            axis=0,
        )
        within[rows] = dot_nn(mixed, stacked)

    for b in range(BLOCKS):
        within_block(b)

    wait(s1.at[pl.ds(0, PLANE - 1)], st_r.at[2])
    running = jnp.zeros((ROWS, W), F32)
    for i in range(PLANE):
        pref[i] = running
        running = running * jnp.exp(t_plane[i]) + s1[i].astype(F32)
    s2_own[...] = running.astype(BF16)

    def send_s2(k, carry):
        @pl.when(z + k < NZ)
        def _():
            send(s2_own, s2.at[z], s2_s.at[k], s2_r.at[z], (z + k, x, c, y))

        return carry

    lax.fori_loop(1, NZ, send_s2, 0)

    @pl.when(c == 1)
    def _():
        wait(wbuf.at[OUT_GATE], dd_r.at[1 + OUT_GATE - NA])
        wait(wbuf.at[pl.ds(0, NA)], dd_r.at[0])

    lax.fori_loop(OUTER, VALUE + 1, project, 0)
    lax.fori_loop(OUT_GATE, OUT_GATE + 1, project, 0)
    product[...] = pj[INNER] * pj[VALUE]
    mixer[...] = (pj[OUTER, RIM : RIM + LEN] * causal(product, gated_taps, 0, W)).astype(BF16)

    def conv_block(b, carry):
        start = pl.multiple_of(b * OWN, OWN)
        conv_part[pl.ds(start, OWN)] = dot_nt(
            mixer[pl.ds(start, OWN)], wbuf[CONV_T].reshape(D, W)
        )
        return carry

    lax.fori_loop(0, NY, conv_block, 0)

    wait(t_z.at[pl.ds(0, NZ - 1)], st_r.at[1])
    zin[...] = jnp.zeros((ROWS, W), F32)

    def take_s2(k, carry):
        @pl.when(k < z)
        def _():
            wait(s2.at[k], s2_r.at[k])
            zin[...] = zin[...] * jnp.exp(t_z[k]) + s2[k].astype(F32)

        return carry

    lax.fori_loop(0, NZ - 1, take_s2, 0)
    arriving = zin[...]
    logs = jnp.zeros((1, W), F32)
    for i in range(PLANE):
        s3_own[i] = (pref[i] + arriving * jnp.exp(logs)).astype(BF16)
        logs = logs + t_plane[i]
    for k in range(1, PLANE):
        q, where = in_plane(k)
        send(s3_own.at[q], s3.at[p], st_s.at[3], st_r.at[3], where)
    s3[p] = s3_own[p]

    lane = iota((1, W), 1) // HEAD_DIM
    direct_row = per_head(direct, lane)
    same_head = (iota((W, W), 0) // HEAD_DIM == iota((W, W), 1) // HEAD_DIM).astype(F32) * (
        1.0 / HEAD_DIM
    )
    gate = silu(pj[OUT_GATE, RIM : RIM + LEN])
    pj[OUT_GATE, RIM : RIM + LEN] = gate

    wait(s3.at[pl.ds(0, PLANE - 1)], st_r.at[3])
    entering = s3[...].reshape(STATE, W).astype(F32)

    def partial(k):
        b = ym(k)
        rows = pl.ds(pl.multiple_of(b * L, L), L)
        enter = (before[b] + jnp.exp(before_log[b]) * entering).astype(BF16)
        head_out = (
            within[rows]
            + dot_nn(rk[rows], enter) * jnp.exp(cumx[b])
            + direct_row * xin[rows]
        )
        gated = head_out * pj[OUT_GATE, pl.ds(pl.multiple_of(RIM + b * L, RIM), L)]
        mean = dot_nn(gated * gated, same_head, HIGH)
        part = (gated * lax.rsqrt(mean + EPS) * head_scale[...].astype(F32).reshape(1, W)).astype(BF16)
        return conv_part[rows] + dot_nt(part, wbuf[STATE_T].reshape(D, W))

    rs_far[...] = partial(2).astype(BF16)
    send(rs_far.at[0:HALF], got_far_l, rs_s.at[0], rs_r.at[0], y_right)
    send(rs_far.at[HALF:OWN], got_far_r, rs_s.at[1], rs_r.at[1], y_left)
    to_right = partial(1)
    rs_right[HALF:OWN] = to_right[HALF:OWN].astype(BF16)
    send(rs_right.at[HALF:OWN], got_left.at[HALF:OWN], rs_s.at[2], rs_r.at[2], y_right)
    to_left = partial(-1)
    rs_left[0:HALF] = to_left[0:HALF].astype(BF16)
    send(rs_left.at[0:HALF], got_right.at[0:HALF], rs_s.at[3], rs_r.at[3], y_left)
    wait(got_far_l, rs_r.at[0])
    rs_right[0:HALF] = (to_right[0:HALF] + got_far_l[...].astype(F32)).astype(BF16)
    send(rs_right.at[0:HALF], got_left.at[0:HALF], rs_s.at[4], rs_r.at[4], y_right)
    wait(got_far_r, rs_r.at[1])
    rs_left[HALF:OWN] = (to_left[HALF:OWN] + got_far_r[...].astype(F32)).astype(BF16)
    send(rs_left.at[HALF:OWN], got_right.at[HALF:OWN], rs_s.at[5], rs_r.at[5], y_left)
    own_sum = partial(0)

    for index, half in ((0, 0), (1, 1), (2, 1), (3, 0)):
        wait(tok_piece(0, half), tok_s.at[index])
    wait(tok_piece(-1, 0), tok_s.at[4])
    wait(tok_piece(1, 1), tok_s.at[5])

    @pl.when(c == 1)
    def _():
        wait(handed, pair_s)

    @pl.when(c == 0)
    def _():
        wait(wbuf.at[pl.ds(0, NA), pl.ds(0, NZ - 1), 0], az_s)
        wait(wbuf.at[pl.ds(0, NA), :, pl.ds(0, 3)], ax_s)
        for k in (1, 2, 3):
            wait(b_block(x), bx_s.at[k])
        wait(wbuf.at[pl.ds(NA, GROUPS - NA), pl.ds(0, NZ - 1)], bz_s)
        wait(wbuf.at[pl.ds(0, NA)], dd_s.at[0])
        for b in range(GROUPS - NA):
            wait(wbuf.at[NA + b], dd_s.at[1 + b])

    @pl.when(sp < NZ * PLANE - 1)
    def _():
        wait(nb.at[pl.ds(LEN, RIM)], rim_s)

    wait(t_plane.at[pl.ds(0, PLANE - 1)], st_s.at[0])
    wait(t_z.at[pl.ds(0, NZ - 1)], st_s.at[1])
    wait(s_own.at[pl.ds(0, PLANE - 1)], st_s.at[2])
    wait(s3_own.at[pl.ds(0, PLANE - 1)], st_s.at[3])

    def left_s2(k, carry):
        @pl.when(z + k < NZ)
        def _():
            wait(s2_own, s2_s.at[k])

        return carry

    lax.fori_loop(1, NZ, left_s2, 0)
    wait(rs_far.at[0:HALF], rs_s.at[0])
    wait(rs_far.at[HALF:OWN], rs_s.at[1])
    wait(rs_right.at[HALF:OWN], rs_s.at[2])
    wait(rs_left.at[0:HALF], rs_s.at[3])
    wait(rs_right.at[0:HALF], rs_s.at[4])
    wait(rs_left.at[HALF:OWN], rs_s.at[5])

    wait(got_left.at[HALF:OWN], rs_r.at[2])
    wait(got_right.at[0:HALF], rs_r.at[3])
    wait(got_left.at[0:HALF], rs_r.at[4])
    wait(got_right.at[HALF:OWN], rs_r.at[5])
    out[...] = (own_sum + got_left[...].astype(F32) + got_right[...].astype(F32)).astype(BF16)


def per_device(
    tokens,
    input_norm_scale,
    outer_gate_weight,
    inner_gate_weight,
    value_weight_matrix,
    output_gate_weight,
    state_input_weight,
    write_key_weight,
    read_key_weight,
    step_size_weight,
    gated_conv_weight,
    input_conv_weight,
    write_conv_weight,
    read_conv_weight,
    step_size_bias,
    log_decay_rate,
    decay_spikes,
    direct_path_weight,
    head_norm_scale,
    conv_output_weight,
    state_output_weight,
):
    vmem = pl.BlockSpec(memory_space=pltpu.VMEM)
    dma = pltpu.SemaphoreType.DMA
    return pl.pallas_call(
        layer_kernel,
        out_shape=jax.ShapeDtypeStruct((OWN, D), BF16),
        in_specs=[pl.BlockSpec(memory_space=pl.ANY)] * 21,
        out_specs=vmem,
        scratch_shapes=[
            pltpu.VMEM((OWN, D), BF16),
            pltpu.VMEM((D,), BF16),
            pltpu.VMEM((HEADS, D), BF16),
            pltpu.VMEM((3, W), BF16),
            pltpu.VMEM((4, W), BF16),
            pltpu.VMEM((4, STATE), BF16),
            pltpu.VMEM((4, STATE), BF16),
            pltpu.SMEM((HEADS,), F32),
            pltpu.SMEM((HEADS,), F32),
            pltpu.VMEM((HEADS, LEN), F32),
            pltpu.SMEM((HEADS,), F32),
            pltpu.VMEM((W,), BF16),
            dma((21,)),
            pltpu.VMEM((GROUPS, ROWS, W), BF16),
            pltpu.VMEM((LEN, D), F32),
            pltpu.VMEM((BLOCKS, 1, W), F32),
            pltpu.VMEM((GROUPS, NZ, NX, NC, ROWS, W), BF16),
            pltpu.VMEM((RIM + LEN, D), BF16),
            pltpu.VMEM((GROUPS, RIM + LEN, W), F32),
            pltpu.VMEM((RIM + LEN, W), F32),
            pltpu.VMEM((LEN, W), BF16),
            pltpu.VMEM((LEN, W), F32),
            pltpu.VMEM((LEN, STATE), BF16),
            pltpu.VMEM((LEN, STATE), BF16),
            pltpu.VMEM((LEN, W), F32),
            pltpu.VMEM((BLOCKS, L, W), F32),
            pltpu.VMEM((BLOCKS, STATE, W), F32),
            pltpu.VMEM((BLOCKS, 1, W), F32),
            pltpu.VMEM((PLANE, ROWS, W), BF16),
            pltpu.VMEM((PLANE, ROWS, W), BF16),
            pltpu.VMEM((PLANE, ROWS, W), F32),
            pltpu.VMEM((ROWS, W), BF16),
            pltpu.VMEM((NZ, ROWS, W), BF16),
            pltpu.VMEM((ROWS, W), F32),
            pltpu.VMEM((PLANE, ROWS, W), BF16),
            pltpu.VMEM((PLANE, ROWS, W), BF16),
            pltpu.VMEM((1, 1, W), F32),
            pltpu.VMEM((PLANE, 1, W), F32),
            pltpu.VMEM((1, 1, W), F32),
            pltpu.VMEM((NZ, 1, W), F32),
            pltpu.VMEM((OWN, D), BF16),
            pltpu.VMEM((OWN, D), BF16),
            pltpu.VMEM((OWN, D), BF16),
            pltpu.VMEM((OWN // 2, D), BF16),
            pltpu.VMEM((OWN // 2, D), BF16),
            pltpu.VMEM((OWN, D), BF16),
            pltpu.VMEM((OWN, D), BF16),
            dma((6,)),
            dma((6,)),
            dma,
            dma((8,)),
            dma((8,)),
            dma,
            dma((18,)),
            dma((18,)),
            dma((18,)),
            dma((18,)),
            dma((4,)),
            dma((4,)),
            dma,
            dma((24,)),
            dma((24,)),
            dma,
            dma,
            dma((4,)),
            dma((4,)),
            dma,
            dma,
            dma((4,)),
            dma((4,)),
            dma((16,)),
            dma((16,)),
            dma((6,)),
            dma((6,)),
        ],
        compiler_params=pltpu.CompilerParams(
            collective_id=0, has_side_effects=True, vmem_limit_bytes=60 * 1024 * 1024
        ),
    )(
        tokens,
        input_norm_scale,
        outer_gate_weight,
        inner_gate_weight,
        value_weight_matrix,
        output_gate_weight,
        state_input_weight,
        write_key_weight,
        read_key_weight,
        step_size_weight.T,
        gated_conv_weight,
        input_conv_weight,
        write_conv_weight,
        read_conv_weight,
        step_size_bias,
        log_decay_rate,
        decay_spikes,
        direct_path_weight,
        head_norm_scale,
        conv_output_weight.T,
        state_output_weight.T,
    )


def solution(mesh):
    torus = Mesh(mesh.devices.reshape(NZ, NX, NC, mesh.shape["tp"]), SP_TP)
    return jax.shard_map(
        per_device,
        mesh=torus,
        in_specs=(
            P(SP_TP, None),
            P(),
            P(SP, "tp"),
            P(SP, "tp"),
            P(SP, "tp"),
            P(SP, "tp"),
            P(SP, "tp"),
            P(SP, "tp"),
            P(SP, "tp"),
            P(None, "tp"),
            P(None, "tp"),
            P(None, "tp"),
            P(None, "tp"),
            P(None, "tp"),
            P("tp"),
            P("tp"),
            P("tp", SP),
            P("tp"),
            P("tp"),
            P("tp", SP),
            P("tp", SP),
        ),
        out_specs=P(SP_TP, None),
        check_vma=False,
    )
```

```python
import functools

import jax
import jax.numpy as jnp
from jax import lax
from jax.experimental import pallas as pl
from jax.experimental.pallas import tpu as pltpu
from jax.sharding import Mesh
from jax.sharding import PartitionSpec as P

SP = ("sp_0", "sp_1", "sp_2")
SP_TP = ("sp_0", "sp_1", "sp_2", "tp")
NZ, NX, NC, NY = 16, 4, 2, 4
PLANE = NX * NC
D = 2048
ROWS = 16
W = 256
STATE = 128
HEADS = 4
HEAD_DIM = 64
OWN = 128
LEN = 512
RIM = 16
L = 128
BLOCKS = LEN // L
NA = 6
HOP = 2
GROUPS = 8
OUTER, INNER, VALUE, CONV_T, STATE_T, OUT_GATE, STATE_IN, KEYS = range(8)
EPS = 1e-05
MESH = pl.DeviceIdType.MESH
F32 = jnp.float32
BF16 = jnp.bfloat16
HIGH = lax.Precision.HIGHEST


def silu(v):
    return v / (1.0 + jnp.exp(-v))


def dot_nn(a, b, precision=None):
    return lax.dot_general(
        a, b, (((1,), (0,)), ((), ())), precision=precision, preferred_element_type=F32
    )


def dot_nt(a, b, precision=None):
    return lax.dot_general(
        a, b, (((1,), (1,)), ((), ())), precision=precision, preferred_element_type=F32
    )


def dot_tn(a, b, precision=None):
    return lax.dot_general(
        a, b, (((0,), (0,)), ((), ())), precision=precision, preferred_element_type=F32
    )


def iota(shape, dim):
    return lax.broadcasted_iota(jnp.int32, shape, dim)


def layer_kernel(
    tok_hbm,
    scale_hbm,
    outer_w,
    inner_w,
    value_w,
    out_gate_w,
    state_in_w,
    write_w,
    read_w,
    step_w_hbm,
    gated_taps_hbm,
    input_taps_hbm,
    write_taps_hbm,
    read_taps_hbm,
    bias_hbm,
    rate_hbm,
    spikes_hbm,
    direct_hbm,
    head_scale_hbm,
    conv_out_w,
    state_out_w,
    out,
    tok,
    scale,
    step_w,
    gated_taps,
    input_taps,
    write_taps,
    read_taps,
    bias,
    rate,
    spikes,
    direct,
    head_scale,
    in_s,
    conv_part,
    before_log,
    wbuf,
    nb,
    pj,
    product,
    mixer,
    xin,
    wk,
    rk,
    within,
    cumx,
    before,
    decay,
    s_own,
    s1,
    pref,
    s2_own,
    s2,
    zin,
    s3_own,
    s3,
    t_own,
    t_plane,
    tz_own,
    t_z,
    rs_far,
    rs_right,
    rs_left,
    got_far_l,
    got_far_r,
    got_left,
    got_right,
    tok_s,
    tok_r,
    az_s,
    azl_r,
    azr_r,
    ax_s,
    axl_r,
    axr_r,
    axfl_r,
    axfr_r,
    bx_s,
    bx_r,
    bz_s,
    bzl_r,
    bzr_r,
    dd_s,
    dd_r,
    rim_s,
    rim_r,
    st_s,
    st_r,
    s2_s,
    s2_r,
    rs_s,
    rs_r,
):
    z = lax.axis_index("sp_0")
    x = lax.axis_index("sp_1")
    c = lax.axis_index("sp_2")
    y = lax.axis_index("tp")
    p = x * NC + c
    sp = z * PLANE + p

    def zm(k):
        return lax.rem(z + (k + NZ), NZ)

    def xm(k):
        return lax.rem(x + (k + NX), NX)

    def ym(k):
        return lax.rem(y + (k + NY), NY)

    def in_plane(k):
        q = lax.rem(p + k, PLANE)
        return q, (z, q // NC, lax.rem(q, NC), y)

    z_right, z_left = (zm(1), x, c, y), (zm(-1), x, c, y)
    x_right, x_left = (z, xm(1), c, y), (z, xm(-1), c, y)
    z_far_right, z_far_left = (zm(HOP), x, c, y), (zm(-HOP), x, c, y)
    x_across = (z, xm(2), c, y)
    y_right, y_left = (z, x, c, ym(1)), (z, x, c, ym(-1))
    partner = (z, x, 1 - c, y)

    def along(k):
        q = lax.rem(sp + (k + NZ * PLANE), NZ * PLANE)
        r = lax.rem(q, PLANE)
        return (q // PLANE, r // NC, lax.rem(r, NC), y)

    weight_copies = [
        pltpu.make_async_copy(ref, wbuf.at[z, x, c, group], in_s.at[group])
        for group, ref in (
            (OUTER, outer_w),
            (INNER, inner_w),
            (VALUE, value_w),
            (CONV_T, conv_out_w),
            (STATE_T, state_out_w),
            (OUT_GATE, out_gate_w),
            (STATE_IN, state_in_w),
        )
    ] + [
        pltpu.make_async_copy(write_w, wbuf.at[z, x, c, KEYS, :, pl.ds(0, STATE)], in_s.at[7]),
        pltpu.make_async_copy(read_w, wbuf.at[z, x, c, KEYS, :, pl.ds(STATE, STATE)], in_s.at[8]),
    ]
    token_copies = [
        pltpu.make_async_copy(tok_hbm, tok, in_s.at[9]),
        pltpu.make_async_copy(scale_hbm, scale, in_s.at[10]),
    ]
    small_copies = [
        pltpu.make_async_copy(src, dst, in_s.at[11 + i])
        for i, (src, dst) in enumerate(
            (
                (step_w_hbm, step_w),
                (gated_taps_hbm, gated_taps),
                (input_taps_hbm, input_taps),
                (write_taps_hbm, write_taps),
                (read_taps_hbm, read_taps),
                (bias_hbm, bias),
                (rate_hbm, rate),
                (spikes_hbm, spikes),
                (direct_hbm, direct),
                (head_scale_hbm, head_scale),
            )
        )
    ]
    for copy in weight_copies + token_copies + small_copies:
        copy.start()

    barrier = pltpu.get_barrier_semaphore()

    def hello(where):
        pl.semaphore_signal(barrier, inc=1, device_id=where, device_id_type=MESH)

    hello(y_right)
    hello(y_left)
    hello(along(-1))

    hello(partner)
    for where in (z_right, z_left, z_far_right, z_far_left, x_right, x_left, x_across):
        hello(where)

    def send(src, dst, s_sem, r_sem, where):
        pltpu.make_async_remote_copy(
            src_ref=src,
            dst_ref=dst,
            send_sem=s_sem,
            recv_sem=r_sem,
            device_id=where,
            device_id_type=MESH,
        ).start()

    def wait(ref, sem):
        pltpu.make_async_copy(ref, ref, sem).wait()

    HALF = OWN // 2

    def tok_piece(k, half):
        start = pl.multiple_of(RIM + ym(k) * OWN + half * HALF, RIM)
        return nb.at[pl.ds(start, HALF)]

    def send_tok(k, half, index, where):
        piece = tok_piece(k, half)
        send(piece, piece, tok_s.at[index], tok_r.at[index], where)

    def a_block(zz, xx):
        return wbuf.at[zz, xx, c, pl.ds(0, NA)]

    def a_half(zz, xx, half):
        return wbuf.at[zz, xx, c, pl.ds(half * (NA // 2), NA // 2)]

    def b_block(xx):
        return wbuf.at[z, xx, c, pl.ds(NA, GROUPS - NA)]

    def b_chunk(group, zz):
        return wbuf.at[zz, :, c, group]

    def goes_right(d):
        return d != HOP - 1 and d < NZ // 2

    def goes_left(d):
        return d != HOP - 1 and d < NZ // 2 - 1

    def z_pass(blk, k, s_sem, l_sem, r_sem, base):
        if k <= 0 and goes_right(-k):
            send(blk, blk, s_sem, l_sem.at[base - k], z_right)
        if k >= 0 and goes_left(k):
            send(blk, blk, s_sem, r_sem.at[base + k], z_left)
        if k == 0:
            send(blk, blk, s_sem, l_sem.at[base + HOP - 1], z_far_right)
            send(blk, blk, s_sem, r_sem.at[base + HOP - 1], z_far_left)

    def z_wait(blk, k, l_sem, r_sem, base):
        wait(blk, l_sem.at[base - k - 1] if k < 0 else r_sem.at[base + k - 1])

    def az_pass(k):
        z_pass(a_block(zm(k), x), k, az_s, azl_r, azr_r, 0)

    def bz_pass(group, k):
        z_pass(b_chunk(group, zm(k)), k, bz_s, bzl_r, bzr_r, (group - NA) * 8)

    def ax_send(k):
        i = k % NZ
        blk = a_block(zm(k), x)
        send(blk, blk, ax_s, axl_r.at[i], x_right)
        send(blk, blk, ax_s, axr_r.at[i], x_left)

    def ax_forward(k):
        i = k % NZ
        wait(a_block(zm(k), xm(-1)), axl_r.at[i])
        half = a_half(zm(k), xm(-1), 0)
        send(half, half, ax_s, axfl_r.at[i], x_right)
        wait(a_block(zm(k), xm(1)), axr_r.at[i])
        half = a_half(zm(k), xm(1), 1)
        send(half, half, ax_s, axfr_r.at[i], x_left)

    def a_across(k):
        i = k % NZ
        if k == LAST:
            wait(a_block(zm(k), xm(-1)), axl_r.at[i])
            wait(a_block(zm(k), xm(1)), axr_r.at[i])
            wait(a_block(zm(k), xm(2)), axfl_r.at[i])
        else:
            wait(a_half(zm(k), xm(2), 0), axfl_r.at[i])
            wait(a_half(zm(k), xm(2), 1), axfr_r.at[i])
        blk = wbuf.at[zm(k), :, c, pl.ds(0, NA)]
        send(blk, blk, dd_s.at[0], dd_r.at[0], partner)

    def b_across(group, k):
        blk = b_chunk(group, zm(k))
        send(blk, blk, dd_s.at[1 + group - NA], dd_r.at[1 + group - NA], partner)

    order_b = (KEYS, STATE_IN)
    LAST = -(NZ // 2)
    rounds = [((0,),)]
    for r in range(1, max(HOP - 1, NZ // 2 - HOP + 1) + 1):
        near = [(-r, r)] if r < HOP else []
        d = r + HOP - 1
        far = [(-d, d) if d < NZ // 2 else (-d,)] if d <= NZ // 2 else []
        rounds.append(tuple(near + far))

    pl.semaphore_wait(barrier, 11)
    for copy in weight_copies:
        copy.wait()
    az_pass(0)
    for k in (1, 3, 2):
        send(b_block(x), b_block(x), bx_s.at[k], bx_r.at[k], (z, xm(k), c, y))
    ax_send(0)

    for copy in token_copies:
        copy.wait()
    token_rows = tok[...].astype(F32)
    scaled = token_rows * lax.rsqrt(
        jnp.mean(token_rows * token_rows, axis=1, keepdims=True) + EPS
    )
    own_row = pl.multiple_of(RIM + y * OWN, RIM)
    nb[pl.ds(own_row, OWN)] = (scaled * scale[...].astype(F32).reshape(1, D)).astype(BF16)
    send_tok(0, 0, 0, y_right)
    send_tok(0, 1, 1, y_left)
    send_tok(0, 1, 2, y_right)
    send_tok(0, 0, 3, y_left)

    for k in (1, 3, 2):
        wait(b_block(xm(-k)), bx_r.at[k])
    for group in order_b:
        bz_pass(group, 0)

    for r in range(1, len(rounds)):
        for pair in rounds[r]:
            for k in pair:
                z_wait(a_block(zm(k), x), k, azl_r, azr_r, 0)
                az_pass(k)
            for k in pair:
                ax_send(k)
                if k == LAST:
                    blk = a_block(zm(k), x)
                    send(blk, blk, ax_s, axfl_r.at[k % NZ], x_across)
            for group in order_b:
                for k in pair:
                    z_wait(b_chunk(group, zm(k)), k, bzl_r, bzr_r, (group - NA) * 8)
                    bz_pass(group, k)
        for pair in rounds[r - 1]:
            for k in pair:
                ax_forward(k)
                for group in order_b:
                    b_across(group, k)
        if r >= 2:
            for pair in rounds[r - 2]:
                for k in pair:
                    a_across(k)
        if r == 2:
            wait(tok_piece(-1, 0), tok_r.at[0])
            send_tok(-1, 0, 4, y_right)
            wait(tok_piece(1, 1), tok_r.at[1])
            send_tok(1, 1, 5, y_left)
    for pair in rounds[-1]:
        for k in pair:
            for group in order_b:
                b_across(group, k)
            if k != LAST:
                ax_forward(k)

    wait(tok_piece(-1, 1), tok_r.at[2])
    wait(tok_piece(1, 0), tok_r.at[3])
    wait(tok_piece(2, 0), tok_r.at[4])
    wait(tok_piece(2, 1), tok_r.at[5])

    @pl.when(sp < NZ * PLANE - 1)
    def _():
        send(nb.at[pl.ds(LEN, RIM)], nb.at[pl.ds(0, RIM)], rim_s, rim_r, along(1))

    @pl.when(sp == 0)
    def _():
        nb[0:RIM] = jnp.zeros((RIM, D), BF16)

    for copy in small_copies:
        copy.wait()

    step_raw = dot_nt(step_w[...], nb[RIM : RIM + LEN])
    head_row = iota((HEADS, LEN), 0)

    def per_head(ref, index):
        return functools.reduce(
            lambda got, h: jnp.where(index == h, ref[h], got),
            range(1, HEADS),
            jnp.full(index.shape, ref[0], F32),
        )

    shifted = step_raw + per_head(bias, head_row)
    step = jnp.maximum(shifted, 0.0) + jnp.log1p(jnp.exp(-jnp.abs(shifted)))
    log_step = step * (-jnp.exp(per_head(rate, head_row))) + spikes[...]
    ramp = (iota((L, L), 0) <= iota((L, L), 1)).astype(F32)
    spread = (iota((HEADS, W), 1) // HEAD_DIM == iota((HEADS, W), 0)).astype(F32)
    total = jnp.zeros((1, W), F32)
    cum_rows = []
    for b in range(BLOCKS):
        rows = dot_nn(log_step[:, b * L : (b + 1) * L], ramp, HIGH)
        cum_rows.append(rows)
        wide = dot_tn(rows, spread, HIGH)
        cumx[b] = wide
        decay[b] = wide[L - 1 : L]
        before_log[b] = total
        total = total + wide[L - 1 : L]
    t_own[0] = total

    for k in range(1, PLANE):
        _, where = in_plane(k)
        send(t_own, t_plane.at[pl.ds(p, 1)], st_s.at[0], st_r.at[0], where)
    t_plane[p] = total

    for pair in rounds[-2]:
        for k in pair:
            a_across(k)

    @pl.when(sp > 0)
    def _():
        wait(nb.at[pl.ds(0, RIM)], rim_r)

    for group in (STATE_IN, KEYS):
        wait(wbuf.at[:, :, 1 - c, group], dd_r.at[1 + group - NA])

    def project(group, carry):
        acc = dot_nn(nb[...], wbuf[:, :, :, group].reshape(D, W))
        pj[group] = acc.astype(BF16).astype(F32)
        return carry

    lax.fori_loop(STATE_IN, KEYS + 1, project, 0)
    for pair in rounds[-1]:
        for k in pair:
            a_across(k)

    def causal(ref, taps, first, last):
        count = taps.shape[0]
        weights = taps[...].astype(F32)
        start = RIM - count + 1
        running = weights[0:1] * ref[start : start + LEN, first:last]
        for k in range(1, count):
            running = running + weights[k : k + 1] * ref[start + k : start + k + LEN, first:last]
        return running

    xin[...] = silu(causal(pj.at[STATE_IN], input_taps, 0, W))
    wk[...] = silu(causal(pj.at[KEYS], write_taps, 0, STATE)).astype(BF16)
    rk[...] = silu(causal(pj.at[KEYS], read_taps, STATE, W)).astype(BF16)

    state = jnp.zeros((STATE, W), F32)
    lane_head = iota((L, W), 1) // HEAD_DIM
    spread_l = (iota((HEADS, HEADS * L), 1) // L == iota((HEADS, HEADS * L), 0)).astype(F32)
    keep = iota((L, HEADS * L), 0) >= lax.rem(iota((L, HEADS * L), 1), L)
    weighted = []
    for b in range(BLOCKS):
        steps = dot_tn(step[:, b * L : (b + 1) * L], spread, HIGH)
        heavy = xin[b * L : (b + 1) * L] * steps
        weighted.append(heavy.astype(BF16))
        to_end = jnp.exp(decay[b] - cumx[b])
        own = dot_tn(wk[b * L : (b + 1) * L], (heavy * to_end).astype(BF16))
        before[b] = state
        state = state * jnp.exp(decay[b]) + own
    s_own[...] = state.astype(BF16).reshape(PLANE, ROWS, W)
    for k in range(1, PLANE):
        q, where = in_plane(k)
        send(s_own.at[q], s1.at[p], st_s.at[2], st_r.at[2], where)
    s1[p] = s_own[p]

    wait(t_plane.at[pl.ds(0, PLANE - 1)], st_r.at[0])
    tz_own[0] = jnp.sum(t_plane[...], axis=0)

    def send_tz(k, carry):
        there = lax.rem(z + k, NZ)
        send(tz_own, t_z.at[pl.ds(z, 1)], st_s.at[1], st_r.at[1], (there, x, c, y))
        return carry

    lax.fori_loop(1, NZ, send_tz, 0)

    def within_block(b):
        rows = slice(b * L, (b + 1) * L)
        scores = dot_nt(rk[rows], wk[rows])
        cols = dot_tn(cum_rows[b], spread_l, HIGH)
        flat = jnp.concatenate([cum_rows[b][h : h + 1] for h in range(HEADS)], axis=1)
        damping = jnp.exp(jnp.where(keep, cols - flat, -jnp.inf))
        mixed = (jnp.concatenate([scores] * HEADS, axis=1) * damping).astype(BF16)
        stacked = jnp.concatenate(
            [jnp.where(lane_head == h, weighted[b], jnp.zeros_like(weighted[b])) for h in range(HEADS)],
            axis=0,
        )
        within[rows] = dot_nn(mixed, stacked)

    for b in range(BLOCKS):
        within_block(b)

    wait(s1.at[pl.ds(0, PLANE - 1)], st_r.at[2])
    running = jnp.zeros((ROWS, W), F32)
    for i in range(PLANE):
        pref[i] = running
        running = running * jnp.exp(t_plane[i]) + s1[i].astype(F32)
    s2_own[...] = running.astype(BF16)

    def send_s2(k, carry):
        @pl.when(z + k < NZ)
        def _():
            send(s2_own, s2.at[z], s2_s.at[k], s2_r.at[z], (z + k, x, c, y))

        return carry

    lax.fori_loop(1, NZ, send_s2, 0)

    wait(wbuf.at[:, :, 1 - c, pl.ds(0, NA)], dd_r.at[0])
    lax.fori_loop(OUTER, VALUE + 1, project, 0)
    lax.fori_loop(OUT_GATE, OUT_GATE + 1, project, 0)
    product[...] = pj[INNER] * pj[VALUE]
    mixer[...] = (pj[OUTER, RIM : RIM + LEN] * causal(product, gated_taps, 0, W)).astype(BF16)

    def conv_block(b, carry):
        start = pl.multiple_of(b * OWN, OWN)
        conv_part[pl.ds(start, OWN)] = dot_nt(
            mixer[pl.ds(start, OWN)], wbuf[:, :, :, CONV_T].reshape(D, W)
        )
        return carry

    lax.fori_loop(0, NY, conv_block, 0)

    wait(t_z.at[pl.ds(0, NZ - 1)], st_r.at[1])
    zin[...] = jnp.zeros((ROWS, W), F32)

    def take_s2(k, carry):
        @pl.when(k < z)
        def _():
            wait(s2.at[k], s2_r.at[k])
            zin[...] = zin[...] * jnp.exp(t_z[k]) + s2[k].astype(F32)

        return carry

    lax.fori_loop(0, NZ - 1, take_s2, 0)
    arriving = zin[...]
    logs = jnp.zeros((1, W), F32)
    for i in range(PLANE):
        s3_own[i] = (pref[i] + arriving * jnp.exp(logs)).astype(BF16)
        logs = logs + t_plane[i]
    for k in range(1, PLANE):
        q, where = in_plane(k)
        send(s3_own.at[q], s3.at[p], st_s.at[3], st_r.at[3], where)
    s3[p] = s3_own[p]

    lane = iota((1, W), 1) // HEAD_DIM
    direct_row = per_head(direct, lane)
    same_head = (iota((W, W), 0) // HEAD_DIM == iota((W, W), 1) // HEAD_DIM).astype(F32) * (
        1.0 / HEAD_DIM
    )
    gate = silu(pj[OUT_GATE, RIM : RIM + LEN])
    pj[OUT_GATE, RIM : RIM + LEN] = gate

    wait(s3.at[pl.ds(0, PLANE - 1)], st_r.at[3])
    entering = s3[...].reshape(STATE, W).astype(F32)

    def partial(k):
        b = ym(k)
        rows = pl.ds(pl.multiple_of(b * L, L), L)
        enter = (before[b] + jnp.exp(before_log[b]) * entering).astype(BF16)
        head_out = (
            within[rows]
            + dot_nn(rk[rows], enter) * jnp.exp(cumx[b])
            + direct_row * xin[rows]
        )
        gated = head_out * pj[OUT_GATE, pl.ds(pl.multiple_of(RIM + b * L, RIM), L)]
        mean = dot_nn(gated * gated, same_head, HIGH)
        part = (gated * lax.rsqrt(mean + EPS) * head_scale[...].astype(F32).reshape(1, W)).astype(BF16)
        return conv_part[rows] + dot_nt(part, wbuf[:, :, :, STATE_T].reshape(D, W))

    rs_far[...] = partial(2).astype(BF16)
    send(rs_far.at[0:HALF], got_far_l, rs_s.at[0], rs_r.at[0], y_right)
    send(rs_far.at[HALF:OWN], got_far_r, rs_s.at[1], rs_r.at[1], y_left)
    to_right = partial(1)
    rs_right[HALF:OWN] = to_right[HALF:OWN].astype(BF16)
    send(rs_right.at[HALF:OWN], got_left.at[HALF:OWN], rs_s.at[2], rs_r.at[2], y_right)
    to_left = partial(-1)
    rs_left[0:HALF] = to_left[0:HALF].astype(BF16)
    send(rs_left.at[0:HALF], got_right.at[0:HALF], rs_s.at[3], rs_r.at[3], y_left)
    wait(got_far_l, rs_r.at[0])
    rs_right[0:HALF] = (to_right[0:HALF] + got_far_l[...].astype(F32)).astype(BF16)
    send(rs_right.at[0:HALF], got_left.at[0:HALF], rs_s.at[4], rs_r.at[4], y_right)
    wait(got_far_r, rs_r.at[1])
    rs_left[HALF:OWN] = (to_left[HALF:OWN] + got_far_r[...].astype(F32)).astype(BF16)
    send(rs_left.at[HALF:OWN], got_right.at[HALF:OWN], rs_s.at[5], rs_r.at[5], y_left)
    mine = partial(0)

    for index, half in ((0, 0), (1, 1), (2, 1), (3, 0)):
        wait(tok_piece(0, half), tok_s.at[index])
    wait(tok_piece(-1, 0), tok_s.at[4])
    wait(tok_piece(1, 1), tok_s.at[5])
    wait(wbuf.at[pl.ds(0, NZ - 1), 0, 0, pl.ds(0, NA)], az_s)
    wait(wbuf.at[:, pl.ds(0, 3), 0, pl.ds(0, NA)], ax_s)
    for k in (1, 2, 3):
        wait(b_block(x), bx_s.at[k])
    wait(wbuf.at[pl.ds(0, NZ - 1), :, 0, pl.ds(NA, GROUPS - NA)], bz_s)
    wait(wbuf.at[:, :, c, pl.ds(0, NA)], dd_s.at[0])
    for b in range(GROUPS - NA):
        wait(wbuf.at[:, :, c, NA + b], dd_s.at[1 + b])

    @pl.when(sp < NZ * PLANE - 1)
    def _():
        wait(nb.at[pl.ds(LEN, RIM)], rim_s)

    wait(t_plane.at[pl.ds(0, PLANE - 1)], st_s.at[0])
    wait(t_z.at[pl.ds(0, NZ - 1)], st_s.at[1])
    wait(s_own.at[pl.ds(0, PLANE - 1)], st_s.at[2])
    wait(s3_own.at[pl.ds(0, PLANE - 1)], st_s.at[3])

    def left_s2(k, carry):
        @pl.when(z + k < NZ)
        def _():
            wait(s2_own, s2_s.at[k])

        return carry

    lax.fori_loop(1, NZ, left_s2, 0)
    wait(rs_far.at[0:HALF], rs_s.at[0])
    wait(rs_far.at[HALF:OWN], rs_s.at[1])
    wait(rs_right.at[HALF:OWN], rs_s.at[2])
    wait(rs_left.at[0:HALF], rs_s.at[3])
    wait(rs_right.at[0:HALF], rs_s.at[4])
    wait(rs_left.at[HALF:OWN], rs_s.at[5])

    wait(got_left.at[HALF:OWN], rs_r.at[2])
    wait(got_right.at[0:HALF], rs_r.at[3])
    wait(got_left.at[0:HALF], rs_r.at[4])
    wait(got_right.at[HALF:OWN], rs_r.at[5])
    out[...] = (mine + got_left[...].astype(F32) + got_right[...].astype(F32)).astype(BF16)


def per_device(
    tokens,
    input_norm_scale,
    outer_gate_weight,
    inner_gate_weight,
    value_weight_matrix,
    output_gate_weight,
    state_input_weight,
    write_key_weight,
    read_key_weight,
    step_size_weight,
    gated_conv_weight,
    input_conv_weight,
    write_conv_weight,
    read_conv_weight,
    step_size_bias,
    log_decay_rate,
    decay_spikes,
    direct_path_weight,
    head_norm_scale,
    conv_output_weight,
    state_output_weight,
):
    vmem = pl.BlockSpec(memory_space=pltpu.VMEM)
    dma = pltpu.SemaphoreType.DMA
    return pl.pallas_call(
        layer_kernel,
        out_shape=jax.ShapeDtypeStruct((OWN, D), BF16),
        in_specs=[pl.BlockSpec(memory_space=pl.ANY)] * 21,
        out_specs=vmem,
        scratch_shapes=[
            pltpu.VMEM((OWN, D), BF16),
            pltpu.VMEM((D,), BF16),
            pltpu.VMEM((HEADS, D), BF16),
            pltpu.VMEM((3, W), BF16),
            pltpu.VMEM((4, W), BF16),
            pltpu.VMEM((4, STATE), BF16),
            pltpu.VMEM((4, STATE), BF16),
            pltpu.SMEM((HEADS,), F32),
            pltpu.SMEM((HEADS,), F32),
            pltpu.VMEM((HEADS, LEN), F32),
            pltpu.SMEM((HEADS,), F32),
            pltpu.VMEM((W,), BF16),
            dma((21,)),
            pltpu.VMEM((LEN, D), F32),
            pltpu.VMEM((BLOCKS, 1, W), F32),
            pltpu.VMEM((NZ, NX, NC, GROUPS, ROWS, W), BF16),
            pltpu.VMEM((RIM + LEN, D), BF16),
            pltpu.VMEM((GROUPS, RIM + LEN, W), F32),
            pltpu.VMEM((RIM + LEN, W), F32),
            pltpu.VMEM((LEN, W), BF16),
            pltpu.VMEM((LEN, W), F32),
            pltpu.VMEM((LEN, STATE), BF16),
            pltpu.VMEM((LEN, STATE), BF16),
            pltpu.VMEM((LEN, W), F32),
            pltpu.VMEM((BLOCKS, L, W), F32),
            pltpu.VMEM((BLOCKS, STATE, W), F32),
            pltpu.VMEM((BLOCKS, 1, W), F32),
            pltpu.VMEM((PLANE, ROWS, W), BF16),
            pltpu.VMEM((PLANE, ROWS, W), BF16),
            pltpu.VMEM((PLANE, ROWS, W), F32),
            pltpu.VMEM((ROWS, W), BF16),
            pltpu.VMEM((NZ, ROWS, W), BF16),
            pltpu.VMEM((ROWS, W), F32),
            pltpu.VMEM((PLANE, ROWS, W), BF16),
            pltpu.VMEM((PLANE, ROWS, W), BF16),
            pltpu.VMEM((1, 1, W), F32),
            pltpu.VMEM((PLANE, 1, W), F32),
            pltpu.VMEM((1, 1, W), F32),
            pltpu.VMEM((NZ, 1, W), F32),
            pltpu.VMEM((OWN, D), BF16),
            pltpu.VMEM((OWN, D), BF16),
            pltpu.VMEM((OWN, D), BF16),
            pltpu.VMEM((OWN // 2, D), BF16),
            pltpu.VMEM((OWN // 2, D), BF16),
            pltpu.VMEM((OWN, D), BF16),
            pltpu.VMEM((OWN, D), BF16),
            dma((6,)),
            dma((6,)),
            dma,
            dma((8,)),
            dma((8,)),
            dma,
            dma((18,)),
            dma((18,)),
            dma((18,)),
            dma((18,)),
            dma((4,)),
            dma((4,)),
            dma,
            dma((16,)),
            dma((16,)),
            dma((4,)),
            dma((4,)),
            dma,
            dma,
            dma((4,)),
            dma((4,)),
            dma((16,)),
            dma((16,)),
            dma((6,)),
            dma((6,)),
        ],
        compiler_params=pltpu.CompilerParams(
            collective_id=0, has_side_effects=True, vmem_limit_bytes=60 * 1024 * 1024
        ),
    )(
        tokens,
        input_norm_scale,
        outer_gate_weight,
        inner_gate_weight,
        value_weight_matrix,
        output_gate_weight,
        state_input_weight,
        write_key_weight,
        read_key_weight,
        step_size_weight.T,
        gated_conv_weight,
        input_conv_weight,
        write_conv_weight,
        read_conv_weight,
        step_size_bias,
        log_decay_rate,
        decay_spikes,
        direct_path_weight,
        head_norm_scale,
        conv_output_weight.T,
        state_output_weight.T,
    )


def solution(mesh):
    torus = Mesh(mesh.devices.reshape(NZ, NX, NC, mesh.shape["tp"]), SP_TP)
    return jax.shard_map(
        per_device,
        mesh=torus,
        in_specs=(
            P(SP_TP, None),
            P(),
            P(SP, "tp"),
            P(SP, "tp"),
            P(SP, "tp"),
            P(SP, "tp"),
            P(SP, "tp"),
            P(SP, "tp"),
            P(SP, "tp"),
            P(None, "tp"),
            P(None, "tp"),
            P(None, "tp"),
            P(None, "tp"),
            P(None, "tp"),
            P("tp"),
            P("tp"),
            P("tp", SP),
            P("tp"),
            P("tp"),
            P("tp", SP),
            P("tp", SP),
        ),
        out_specs=P(SP_TP, None),
        check_vma=False,
    )
```

```python
import functools

import jax
import jax.numpy as jnp
from jax import lax
from jax.experimental import pallas as pl
from jax.experimental.pallas import tpu as pltpu
from jax.sharding import Mesh
from jax.sharding import PartitionSpec as P

SP = ("sp_0", "sp_1", "sp_2")
SP_TP = ("sp_0", "sp_1", "sp_2", "tp")
NZ, NX, NC, NY = 16, 4, 2, 4
PLANE = NX * NC
D = 2048
ROWS = 16
W = 256
STATE = 128
HEADS = 4
HEAD_DIM = 64
OWN = 128
LEN = 512
RIM = 16
L = 128
BLOCKS = LEN // L
NA = 6
GROUPS = 8
OUTER, INNER, VALUE, CONV_T, STATE_T, OUT_GATE, STATE_IN, KEYS = range(8)
EPS = 1e-05
MESH = pl.DeviceIdType.MESH
F32 = jnp.float32
BF16 = jnp.bfloat16
HIGH = lax.Precision.HIGHEST


def silu(v):
    return v / (1.0 + jnp.exp(-v))


def dot_nn(a, b, precision=None):
    return lax.dot_general(
        a, b, (((1,), (0,)), ((), ())), precision=precision, preferred_element_type=F32
    )


def dot_nt(a, b, precision=None):
    return lax.dot_general(
        a, b, (((1,), (1,)), ((), ())), precision=precision, preferred_element_type=F32
    )


def dot_tn(a, b, precision=None):
    return lax.dot_general(
        a, b, (((0,), (0,)), ((), ())), precision=precision, preferred_element_type=F32
    )


def iota(shape, dim):
    return lax.broadcasted_iota(jnp.int32, shape, dim)


def layer_kernel(
    tok_hbm,
    scale_hbm,
    outer_w,
    inner_w,
    value_w,
    out_gate_w,
    state_in_w,
    write_w,
    read_w,
    step_w_hbm,
    gated_taps_hbm,
    input_taps_hbm,
    write_taps_hbm,
    read_taps_hbm,
    bias_hbm,
    rate_hbm,
    spikes_hbm,
    direct_hbm,
    head_scale_hbm,
    conv_out_w,
    state_out_w,
    out,
    tok,
    scale,
    step_w,
    gated_taps,
    input_taps,
    write_taps,
    read_taps,
    bias,
    rate,
    spikes,
    direct,
    head_scale,
    in_s,
    conv_part,
    before_log,
    wbuf,
    nb,
    pj,
    product,
    mixer,
    xin,
    wk,
    rk,
    within,
    cumx,
    before,
    decay,
    s_own,
    s1,
    pref,
    s2_own,
    s2,
    zin,
    s3_own,
    s3,
    t_own,
    t_plane,
    tz_own,
    t_z,
    rs_far,
    rs_right,
    rs_left,
    got_far_l,
    got_far_r,
    got_left,
    got_right,
    tok_s,
    tok_r,
    az_s,
    azl_r,
    azr_r,
    ax_s,
    axl_r,
    axr_r,
    axfl_r,
    axfr_r,
    bx_s,
    bx_r,
    bz_s,
    bzl_r,
    bzr_r,
    dd_s,
    dd_r,
    rim_s,
    rim_r,
    st_s,
    st_r,
    s2_s,
    s2_r,
    rs_s,
    rs_r,
):
    z = lax.axis_index("sp_0")
    x = lax.axis_index("sp_1")
    c = lax.axis_index("sp_2")
    y = lax.axis_index("tp")
    p = x * NC + c
    sp = z * PLANE + p

    def zm(k):
        return lax.rem(z + (k + NZ), NZ)

    def xm(k):
        return lax.rem(x + (k + NX), NX)

    def ym(k):
        return lax.rem(y + (k + NY), NY)

    def in_plane(k):
        q = lax.rem(p + k, PLANE)
        return q, (z, q // NC, lax.rem(q, NC), y)

    z_right, z_left = (zm(1), x, c, y), (zm(-1), x, c, y)
    x_right, x_left = (z, xm(1), c, y), (z, xm(-1), c, y)
    x_across = (z, xm(2), c, y)
    y_right, y_left = (z, x, c, ym(1)), (z, x, c, ym(-1))
    partner = (z, x, 1 - c, y)

    def along(k):
        q = lax.rem(sp + (k + NZ * PLANE), NZ * PLANE)
        r = lax.rem(q, PLANE)
        return (q // PLANE, r // NC, lax.rem(r, NC), y)

    weight_copies = [
        pltpu.make_async_copy(ref, wbuf.at[z, x, c, group], in_s.at[group])
        for group, ref in (
            (OUTER, outer_w),
            (INNER, inner_w),
            (VALUE, value_w),
            (CONV_T, conv_out_w),
            (STATE_T, state_out_w),
            (OUT_GATE, out_gate_w),
            (STATE_IN, state_in_w),
        )
    ] + [
        pltpu.make_async_copy(write_w, wbuf.at[z, x, c, KEYS, :, pl.ds(0, STATE)], in_s.at[7]),
        pltpu.make_async_copy(read_w, wbuf.at[z, x, c, KEYS, :, pl.ds(STATE, STATE)], in_s.at[8]),
    ]
    token_copies = [
        pltpu.make_async_copy(tok_hbm, tok, in_s.at[9]),
        pltpu.make_async_copy(scale_hbm, scale, in_s.at[10]),
    ]
    small_copies = [
        pltpu.make_async_copy(src, dst, in_s.at[11 + i])
        for i, (src, dst) in enumerate(
            (
                (step_w_hbm, step_w),
                (gated_taps_hbm, gated_taps),
                (input_taps_hbm, input_taps),
                (write_taps_hbm, write_taps),
                (read_taps_hbm, read_taps),
                (bias_hbm, bias),
                (rate_hbm, rate),
                (spikes_hbm, spikes),
                (direct_hbm, direct),
                (head_scale_hbm, head_scale),
            )
        )
    ]
    for copy in weight_copies + token_copies + small_copies:
        copy.start()

    barrier = pltpu.get_barrier_semaphore()

    def hello(where):
        pl.semaphore_signal(barrier, inc=1, device_id=where, device_id_type=MESH)

    hello(y_right)
    hello(y_left)
    hello(along(-1))

    hello(partner)
    for where in (z_right, z_left, x_right, x_left, x_across):
        hello(where)

    def send(src, dst, s_sem, r_sem, where):
        pltpu.make_async_remote_copy(
            src_ref=src,
            dst_ref=dst,
            send_sem=s_sem,
            recv_sem=r_sem,
            device_id=where,
            device_id_type=MESH,
        ).start()

    def wait(ref, sem):
        pltpu.make_async_copy(ref, ref, sem).wait()

    HALF = OWN // 2

    def tok_piece(k, half):
        start = pl.multiple_of(RIM + ym(k) * OWN + half * HALF, RIM)
        return nb.at[pl.ds(start, HALF)]

    def send_tok(k, half, index, where):
        piece = tok_piece(k, half)
        send(piece, piece, tok_s.at[index], tok_r.at[index], where)

    def a_block(zz, xx):
        return wbuf.at[zz, xx, c, pl.ds(0, NA)]

    def a_half(zz, xx, half):
        return wbuf.at[zz, xx, c, pl.ds(half * (NA // 2), NA // 2)]

    def b_block(xx):
        return wbuf.at[z, xx, c, pl.ds(NA, GROUPS - NA)]

    def b_chunk(group, zz):
        return wbuf.at[zz, :, c, group]

    def goes_right(d):
        return d < NZ // 2

    def goes_left(d):
        return d < NZ // 2 - 1

    def z_pass(blk, k, s_sem, l_sem, r_sem, base):
        if k <= 0 and goes_right(-k):
            send(blk, blk, s_sem, l_sem.at[base - k], z_right)
        if k >= 0 and goes_left(k):
            send(blk, blk, s_sem, r_sem.at[base + k], z_left)

    def z_wait(blk, k, l_sem, r_sem, base):
        wait(blk, l_sem.at[base - k - 1] if k < 0 else r_sem.at[base + k - 1])

    def az_pass(k):
        z_pass(a_block(zm(k), x), k, az_s, azl_r, azr_r, 0)

    def bz_pass(group, k):
        z_pass(b_chunk(group, zm(k)), k, bz_s, bzl_r, bzr_r, (group - NA) * 8)

    def ax_send(k):
        i = k % NZ
        blk = a_block(zm(k), x)
        send(blk, blk, ax_s, axl_r.at[i], x_right)
        send(blk, blk, ax_s, axr_r.at[i], x_left)

    def ax_forward(k):
        i = k % NZ
        wait(a_block(zm(k), xm(-1)), axl_r.at[i])
        half = a_half(zm(k), xm(-1), 0)
        send(half, half, ax_s, axfl_r.at[i], x_right)
        wait(a_block(zm(k), xm(1)), axr_r.at[i])
        half = a_half(zm(k), xm(1), 1)
        send(half, half, ax_s, axfr_r.at[i], x_left)

    def a_across(k):
        i = k % NZ
        if k == LAST:
            wait(a_block(zm(k), xm(-1)), axl_r.at[i])
            wait(a_block(zm(k), xm(1)), axr_r.at[i])
            wait(a_block(zm(k), xm(2)), axfl_r.at[i])
        else:
            wait(a_half(zm(k), xm(2), 0), axfl_r.at[i])
            wait(a_half(zm(k), xm(2), 1), axfr_r.at[i])
        blk = wbuf.at[zm(k), :, c, pl.ds(0, NA)]
        send(blk, blk, dd_s.at[0], dd_r.at[0], partner)

    def b_across(group, k):
        blk = b_chunk(group, zm(k))
        send(blk, blk, dd_s.at[1 + group - NA], dd_r.at[1 + group - NA], partner)

    order_b = (KEYS, STATE_IN)
    LAST = -(NZ // 2)
    rounds = [((0,),)]
    for r in range(1, 9):
        rounds.append((((-r, r) if r < 8 else (-r,)),))

    pl.semaphore_wait(barrier, 9)
    for copy in weight_copies:
        copy.wait()
    az_pass(0)
    for k in (1, 3, 2):
        send(b_block(x), b_block(x), bx_s.at[k], bx_r.at[k], (z, xm(k), c, y))
    ax_send(0)

    for copy in token_copies:
        copy.wait()
    token_rows = tok[...].astype(F32)
    scaled = token_rows * lax.rsqrt(
        jnp.mean(token_rows * token_rows, axis=1, keepdims=True) + EPS
    )
    own_row = pl.multiple_of(RIM + y * OWN, RIM)
    nb[pl.ds(own_row, OWN)] = (scaled * scale[...].astype(F32).reshape(1, D)).astype(BF16)
    send_tok(0, 0, 0, y_right)
    send_tok(0, 1, 1, y_left)
    send_tok(0, 1, 2, y_right)
    send_tok(0, 0, 3, y_left)

    for k in (1, 3, 2):
        wait(b_block(xm(-k)), bx_r.at[k])
    for group in order_b:
        bz_pass(group, 0)

    for r in range(1, len(rounds)):
        for pair in rounds[r]:
            for k in pair:
                z_wait(a_block(zm(k), x), k, azl_r, azr_r, 0)
                az_pass(k)
            for k in pair:
                ax_send(k)
                if k == LAST:
                    blk = a_block(zm(k), x)
                    send(blk, blk, ax_s, axfl_r.at[k % NZ], x_across)
            for group in order_b:
                for k in pair:
                    z_wait(b_chunk(group, zm(k)), k, bzl_r, bzr_r, (group - NA) * 8)
                    bz_pass(group, k)
        for pair in rounds[r - 1]:
            for k in pair:
                ax_forward(k)
                for group in order_b:
                    b_across(group, k)
        if r >= 2:
            for pair in rounds[r - 2]:
                for k in pair:
                    a_across(k)
        if r == 2:
            wait(tok_piece(-1, 0), tok_r.at[0])
            send_tok(-1, 0, 4, y_right)
            wait(tok_piece(1, 1), tok_r.at[1])
            send_tok(1, 1, 5, y_left)
    for pair in rounds[-1]:
        for k in pair:
            for group in order_b:
                b_across(group, k)
            if k != LAST:
                ax_forward(k)

    wait(tok_piece(-1, 1), tok_r.at[2])
    wait(tok_piece(1, 0), tok_r.at[3])
    wait(tok_piece(2, 0), tok_r.at[4])
    wait(tok_piece(2, 1), tok_r.at[5])

    @pl.when(sp < NZ * PLANE - 1)
    def _():
        send(nb.at[pl.ds(LEN, RIM)], nb.at[pl.ds(0, RIM)], rim_s, rim_r, along(1))

    @pl.when(sp == 0)
    def _():
        nb[0:RIM] = jnp.zeros((RIM, D), BF16)

    for copy in small_copies:
        copy.wait()

    step_raw = dot_nt(step_w[...], nb[RIM : RIM + LEN])
    head_row = iota((HEADS, LEN), 0)

    def per_head(ref, index):
        return functools.reduce(
            lambda got, h: jnp.where(index == h, ref[h], got),
            range(1, HEADS),
            jnp.full(index.shape, ref[0], F32),
        )

    shifted = step_raw + per_head(bias, head_row)
    step = jnp.maximum(shifted, 0.0) + jnp.log1p(jnp.exp(-jnp.abs(shifted)))
    log_step = step * (-jnp.exp(per_head(rate, head_row))) + spikes[...]
    ramp = (iota((L, L), 0) <= iota((L, L), 1)).astype(F32)
    spread = (iota((HEADS, W), 1) // HEAD_DIM == iota((HEADS, W), 0)).astype(F32)
    total = jnp.zeros((1, W), F32)
    cum_rows = []
    for b in range(BLOCKS):
        rows = dot_nn(log_step[:, b * L : (b + 1) * L], ramp, HIGH)
        cum_rows.append(rows)
        wide = dot_tn(rows, spread, HIGH)
        cumx[b] = wide
        decay[b] = wide[L - 1 : L]
        before_log[b] = total
        total = total + wide[L - 1 : L]
    t_own[0] = total

    for k in range(1, PLANE):
        _, where = in_plane(k)
        send(t_own, t_plane.at[pl.ds(p, 1)], st_s.at[0], st_r.at[0], where)
    t_plane[p] = total

    for pair in rounds[-2]:
        for k in pair:
            a_across(k)

    @pl.when(sp > 0)
    def _():
        wait(nb.at[pl.ds(0, RIM)], rim_r)

    for group in (STATE_IN, KEYS):
        wait(wbuf.at[:, :, 1 - c, group], dd_r.at[1 + group - NA])

    def project(group, carry):
        acc = dot_nn(nb[...], wbuf[:, :, :, group].reshape(D, W))
        pj[group] = acc.astype(BF16).astype(F32)
        return carry

    lax.fori_loop(STATE_IN, KEYS + 1, project, 0)
    for pair in rounds[-1]:
        for k in pair:
            a_across(k)

    def causal(ref, taps, first, last):
        count = taps.shape[0]
        weights = taps[...].astype(F32)
        start = RIM - count + 1
        running = weights[0:1] * ref[start : start + LEN, first:last]
        for k in range(1, count):
            running = running + weights[k : k + 1] * ref[start + k : start + k + LEN, first:last]
        return running

    xin[...] = silu(causal(pj.at[STATE_IN], input_taps, 0, W))
    wk[...] = silu(causal(pj.at[KEYS], write_taps, 0, STATE)).astype(BF16)
    rk[...] = silu(causal(pj.at[KEYS], read_taps, STATE, W)).astype(BF16)

    state = jnp.zeros((STATE, W), F32)
    lane_head = iota((L, W), 1) // HEAD_DIM
    spread_l = (iota((HEADS, HEADS * L), 1) // L == iota((HEADS, HEADS * L), 0)).astype(F32)
    keep = iota((L, HEADS * L), 0) >= lax.rem(iota((L, HEADS * L), 1), L)
    weighted = []
    for b in range(BLOCKS):
        steps = dot_tn(step[:, b * L : (b + 1) * L], spread, HIGH)
        heavy = xin[b * L : (b + 1) * L] * steps
        weighted.append(heavy.astype(BF16))
        to_end = jnp.exp(decay[b] - cumx[b])
        own = dot_tn(wk[b * L : (b + 1) * L], (heavy * to_end).astype(BF16))
        before[b] = state
        state = state * jnp.exp(decay[b]) + own
    s_own[...] = state.astype(BF16).reshape(PLANE, ROWS, W)
    for k in range(1, PLANE):
        q, where = in_plane(k)
        send(s_own.at[q], s1.at[p], st_s.at[2], st_r.at[2], where)
    s1[p] = s_own[p]

    wait(t_plane.at[pl.ds(0, PLANE - 1)], st_r.at[0])
    tz_own[0] = jnp.sum(t_plane[...], axis=0)

    def send_tz(k, carry):
        there = lax.rem(z + k, NZ)
        send(tz_own, t_z.at[pl.ds(z, 1)], st_s.at[1], st_r.at[1], (there, x, c, y))
        return carry

    lax.fori_loop(1, NZ, send_tz, 0)

    def within_block(b):
        rows = slice(b * L, (b + 1) * L)
        scores = dot_nt(rk[rows], wk[rows])
        cols = dot_tn(cum_rows[b], spread_l, HIGH)
        flat = jnp.concatenate([cum_rows[b][h : h + 1] for h in range(HEADS)], axis=1)
        damping = jnp.exp(jnp.where(keep, cols - flat, -jnp.inf))
        mixed = (jnp.concatenate([scores] * HEADS, axis=1) * damping).astype(BF16)
        stacked = jnp.concatenate(
            [jnp.where(lane_head == h, weighted[b], jnp.zeros_like(weighted[b])) for h in range(HEADS)],
            axis=0,
        )
        within[rows] = dot_nn(mixed, stacked)

    for b in range(BLOCKS):
        within_block(b)

    wait(s1.at[pl.ds(0, PLANE - 1)], st_r.at[2])
    running = jnp.zeros((ROWS, W), F32)
    for i in range(PLANE):
        pref[i] = running
        running = running * jnp.exp(t_plane[i]) + s1[i].astype(F32)
    s2_own[...] = running.astype(BF16)

    def send_s2(k, carry):
        @pl.when(z + k < NZ)
        def _():
            send(s2_own, s2.at[z], s2_s.at[k], s2_r.at[z], (z + k, x, c, y))

        return carry

    lax.fori_loop(1, NZ, send_s2, 0)

    wait(wbuf.at[:, :, 1 - c, pl.ds(0, NA)], dd_r.at[0])
    lax.fori_loop(OUTER, VALUE + 1, project, 0)
    lax.fori_loop(OUT_GATE, OUT_GATE + 1, project, 0)
    product[...] = pj[INNER] * pj[VALUE]
    mixer[...] = (pj[OUTER, RIM : RIM + LEN] * causal(product, gated_taps, 0, W)).astype(BF16)

    def conv_block(b, carry):
        start = pl.multiple_of(b * OWN, OWN)
        conv_part[pl.ds(start, OWN)] = dot_nt(
            mixer[pl.ds(start, OWN)], wbuf[:, :, :, CONV_T].reshape(D, W)
        )
        return carry

    lax.fori_loop(0, NY, conv_block, 0)

    wait(t_z.at[pl.ds(0, NZ - 1)], st_r.at[1])
    zin[...] = jnp.zeros((ROWS, W), F32)

    def take_s2(k, carry):
        @pl.when(k < z)
        def _():
            wait(s2.at[k], s2_r.at[k])
            zin[...] = zin[...] * jnp.exp(t_z[k]) + s2[k].astype(F32)

        return carry

    lax.fori_loop(0, NZ - 1, take_s2, 0)
    arriving = zin[...]
    logs = jnp.zeros((1, W), F32)
    for i in range(PLANE):
        s3_own[i] = (pref[i] + arriving * jnp.exp(logs)).astype(BF16)
        logs = logs + t_plane[i]
    for k in range(1, PLANE):
        q, where = in_plane(k)
        send(s3_own.at[q], s3.at[p], st_s.at[3], st_r.at[3], where)
    s3[p] = s3_own[p]

    lane = iota((1, W), 1) // HEAD_DIM
    direct_row = per_head(direct, lane)
    same_head = (iota((W, W), 0) // HEAD_DIM == iota((W, W), 1) // HEAD_DIM).astype(F32) * (
        1.0 / HEAD_DIM
    )
    gate = silu(pj[OUT_GATE, RIM : RIM + LEN])
    pj[OUT_GATE, RIM : RIM + LEN] = gate

    wait(s3.at[pl.ds(0, PLANE - 1)], st_r.at[3])
    entering = s3[...].reshape(STATE, W).astype(F32)

    def partial(k):
        b = ym(k)
        rows = pl.ds(pl.multiple_of(b * L, L), L)
        enter = (before[b] + jnp.exp(before_log[b]) * entering).astype(BF16)
        head_out = (
            within[rows]
            + dot_nn(rk[rows], enter) * jnp.exp(cumx[b])
            + direct_row * xin[rows]
        )
        gated = head_out * pj[OUT_GATE, pl.ds(pl.multiple_of(RIM + b * L, RIM), L)]
        mean = dot_nn(gated * gated, same_head, HIGH)
        part = (gated * lax.rsqrt(mean + EPS) * head_scale[...].astype(F32).reshape(1, W)).astype(BF16)
        return conv_part[rows] + dot_nt(part, wbuf[:, :, :, STATE_T].reshape(D, W))

    rs_far[...] = partial(2).astype(BF16)
    send(rs_far.at[0:HALF], got_far_l, rs_s.at[0], rs_r.at[0], y_right)
    send(rs_far.at[HALF:OWN], got_far_r, rs_s.at[1], rs_r.at[1], y_left)
    to_right = partial(1)
    rs_right[HALF:OWN] = to_right[HALF:OWN].astype(BF16)
    send(rs_right.at[HALF:OWN], got_left.at[HALF:OWN], rs_s.at[2], rs_r.at[2], y_right)
    to_left = partial(-1)
    rs_left[0:HALF] = to_left[0:HALF].astype(BF16)
    send(rs_left.at[0:HALF], got_right.at[0:HALF], rs_s.at[3], rs_r.at[3], y_left)
    wait(got_far_l, rs_r.at[0])
    rs_right[0:HALF] = (to_right[0:HALF] + got_far_l[...].astype(F32)).astype(BF16)
    send(rs_right.at[0:HALF], got_left.at[0:HALF], rs_s.at[4], rs_r.at[4], y_right)
    wait(got_far_r, rs_r.at[1])
    rs_left[HALF:OWN] = (to_left[HALF:OWN] + got_far_r[...].astype(F32)).astype(BF16)
    send(rs_left.at[HALF:OWN], got_right.at[HALF:OWN], rs_s.at[5], rs_r.at[5], y_left)
    mine = partial(0)

    for index, half in ((0, 0), (1, 1), (2, 1), (3, 0)):
        wait(tok_piece(0, half), tok_s.at[index])
    wait(tok_piece(-1, 0), tok_s.at[4])
    wait(tok_piece(1, 1), tok_s.at[5])
    wait(wbuf.at[pl.ds(0, NZ - 1), 0, 0, pl.ds(0, NA)], az_s)
    wait(wbuf.at[:, pl.ds(0, 3), 0, pl.ds(0, NA)], ax_s)
    for k in (1, 2, 3):
        wait(b_block(x), bx_s.at[k])
    wait(wbuf.at[pl.ds(0, NZ - 1), :, 0, pl.ds(NA, GROUPS - NA)], bz_s)
    wait(wbuf.at[:, :, c, pl.ds(0, NA)], dd_s.at[0])
    for b in range(GROUPS - NA):
        wait(wbuf.at[:, :, c, NA + b], dd_s.at[1 + b])

    @pl.when(sp < NZ * PLANE - 1)
    def _():
        wait(nb.at[pl.ds(LEN, RIM)], rim_s)

    wait(t_plane.at[pl.ds(0, PLANE - 1)], st_s.at[0])
    wait(t_z.at[pl.ds(0, NZ - 1)], st_s.at[1])
    wait(s_own.at[pl.ds(0, PLANE - 1)], st_s.at[2])
    wait(s3_own.at[pl.ds(0, PLANE - 1)], st_s.at[3])

    def left_s2(k, carry):
        @pl.when(z + k < NZ)
        def _():
            wait(s2_own, s2_s.at[k])

        return carry

    lax.fori_loop(1, NZ, left_s2, 0)
    wait(rs_far.at[0:HALF], rs_s.at[0])
    wait(rs_far.at[HALF:OWN], rs_s.at[1])
    wait(rs_right.at[HALF:OWN], rs_s.at[2])
    wait(rs_left.at[0:HALF], rs_s.at[3])
    wait(rs_right.at[0:HALF], rs_s.at[4])
    wait(rs_left.at[HALF:OWN], rs_s.at[5])

    wait(got_left.at[HALF:OWN], rs_r.at[2])
    wait(got_right.at[0:HALF], rs_r.at[3])
    wait(got_left.at[0:HALF], rs_r.at[4])
    wait(got_right.at[HALF:OWN], rs_r.at[5])
    out[...] = (mine + got_left[...].astype(F32) + got_right[...].astype(F32)).astype(BF16)


def per_device(
    tokens,
    input_norm_scale,
    outer_gate_weight,
    inner_gate_weight,
    value_weight_matrix,
    output_gate_weight,
    state_input_weight,
    write_key_weight,
    read_key_weight,
    step_size_weight,
    gated_conv_weight,
    input_conv_weight,
    write_conv_weight,
    read_conv_weight,
    step_size_bias,
    log_decay_rate,
    decay_spikes,
    direct_path_weight,
    head_norm_scale,
    conv_output_weight,
    state_output_weight,
):
    vmem = pl.BlockSpec(memory_space=pltpu.VMEM)
    dma = pltpu.SemaphoreType.DMA
    return pl.pallas_call(
        layer_kernel,
        out_shape=jax.ShapeDtypeStruct((OWN, D), BF16),
        in_specs=[pl.BlockSpec(memory_space=pl.ANY)] * 21,
        out_specs=vmem,
        scratch_shapes=[
            pltpu.VMEM((OWN, D), BF16),
            pltpu.VMEM((D,), BF16),
            pltpu.VMEM((HEADS, D), BF16),
            pltpu.VMEM((3, W), BF16),
            pltpu.VMEM((4, W), BF16),
            pltpu.VMEM((4, STATE), BF16),
            pltpu.VMEM((4, STATE), BF16),
            pltpu.SMEM((HEADS,), F32),
            pltpu.SMEM((HEADS,), F32),
            pltpu.VMEM((HEADS, LEN), F32),
            pltpu.SMEM((HEADS,), F32),
            pltpu.VMEM((W,), BF16),
            dma((21,)),
            pltpu.VMEM((LEN, D), F32),
            pltpu.VMEM((BLOCKS, 1, W), F32),
            pltpu.VMEM((NZ, NX, NC, GROUPS, ROWS, W), BF16),
            pltpu.VMEM((RIM + LEN, D), BF16),
            pltpu.VMEM((GROUPS, RIM + LEN, W), F32),
            pltpu.VMEM((RIM + LEN, W), F32),
            pltpu.VMEM((LEN, W), BF16),
            pltpu.VMEM((LEN, W), F32),
            pltpu.VMEM((LEN, STATE), BF16),
            pltpu.VMEM((LEN, STATE), BF16),
            pltpu.VMEM((LEN, W), F32),
            pltpu.VMEM((BLOCKS, L, W), F32),
            pltpu.VMEM((BLOCKS, STATE, W), F32),
            pltpu.VMEM((BLOCKS, 1, W), F32),
            pltpu.VMEM((PLANE, ROWS, W), BF16),
            pltpu.VMEM((PLANE, ROWS, W), BF16),
            pltpu.VMEM((PLANE, ROWS, W), F32),
            pltpu.VMEM((ROWS, W), BF16),
            pltpu.VMEM((NZ, ROWS, W), BF16),
            pltpu.VMEM((ROWS, W), F32),
            pltpu.VMEM((PLANE, ROWS, W), BF16),
            pltpu.VMEM((PLANE, ROWS, W), BF16),
            pltpu.VMEM((1, 1, W), F32),
            pltpu.VMEM((PLANE, 1, W), F32),
            pltpu.VMEM((1, 1, W), F32),
            pltpu.VMEM((NZ, 1, W), F32),
            pltpu.VMEM((OWN, D), BF16),
            pltpu.VMEM((OWN, D), BF16),
            pltpu.VMEM((OWN, D), BF16),
            pltpu.VMEM((OWN // 2, D), BF16),
            pltpu.VMEM((OWN // 2, D), BF16),
            pltpu.VMEM((OWN, D), BF16),
            pltpu.VMEM((OWN, D), BF16),
            dma((6,)),
            dma((6,)),
            dma,
            dma((8,)),
            dma((8,)),
            dma,
            dma((18,)),
            dma((18,)),
            dma((18,)),
            dma((18,)),
            dma((4,)),
            dma((4,)),
            dma,
            dma((16,)),
            dma((16,)),
            dma((4,)),
            dma((4,)),
            dma,
            dma,
            dma((4,)),
            dma((4,)),
            dma((16,)),
            dma((16,)),
            dma((6,)),
            dma((6,)),
        ],
        compiler_params=pltpu.CompilerParams(
            collective_id=0, has_side_effects=True, vmem_limit_bytes=60 * 1024 * 1024
        ),
    )(
        tokens,
        input_norm_scale,
        outer_gate_weight,
        inner_gate_weight,
        value_weight_matrix,
        output_gate_weight,
        state_input_weight,
        write_key_weight,
        read_key_weight,
        step_size_weight.T,
        gated_conv_weight,
        input_conv_weight,
        write_conv_weight,
        read_conv_weight,
        step_size_bias,
        log_decay_rate,
        decay_spikes,
        direct_path_weight,
        head_norm_scale,
        conv_output_weight.T,
        state_output_weight.T,
    )


def solution(mesh):
    torus = Mesh(mesh.devices.reshape(NZ, NX, NC, mesh.shape["tp"]), SP_TP)
    return jax.shard_map(
        per_device,
        mesh=torus,
        in_specs=(
            P(SP_TP, None),
            P(),
            P(SP, "tp"),
            P(SP, "tp"),
            P(SP, "tp"),
            P(SP, "tp"),
            P(SP, "tp"),
            P(SP, "tp"),
            P(SP, "tp"),
            P(None, "tp"),
            P(None, "tp"),
            P(None, "tp"),
            P(None, "tp"),
            P(None, "tp"),
            P("tp"),
            P("tp"),
            P("tp", SP),
            P("tp"),
            P("tp"),
            P("tp", SP),
            P("tp", SP),
        ),
        out_specs=P(SP_TP, None),
        check_vma=False,
    )
```
